256 devices in a mesh: sp: 16 (over y, x), tp: 16 (over z, core).
Axes of the slice: x: 4, y: 4, z: 8, core: 2. Of those that a mesh axis runs over, the one named last changes fastest.
Arguments:
- resid: bfloat16 [8192, 2048], P(('sp', 'tp')), may hold values from -6 to 6
- query_a: bfloat16 [8192, 16, 128], P('sp', 'tp'), may hold values from -16 to 16
- key_a: bfloat16 [8192, 16, 128], P('sp', 'tp'), may hold values from -16 to 16
- value_a: bfloat16 [8192, 16, 128], P('sp', 'tp'), may hold values from -6 to 6
- query_b: bfloat16 [8192, 16, 64], P('sp', 'tp'), may hold values from -16 to 16
- key_b: bfloat16 [8192, 16, 64], P('sp', 'tp'), may hold values from -16 to 16
- value_b: bfloat16 [8192, 16, 64], P('sp', 'tp'), may hold values from -6 to 6
- mix_a: float32 [16], P('tp'), may hold values from 0.3 to 0.8
- mix_b: float32 [16], P('tp'), may hold values from 0.3 to 0.8
- head_gain_a: float32 [128], replicated, may hold values from 0.1 to 1.9
- head_gain_b: float32 [64], replicated, may hold values from 0.1 to 1.9
- proj_a: bfloat16 [2048, 2048], P('tp'), may hold values from -0.109375 to 0.109375
- proj_b: bfloat16 [1024, 2048], P('tp'), may hold values from -0.109375 to 0.109375
- norm_gain: float32 [2048], replicated, may hold values from 0.1 to 1.9
- route_ids: int32 [8192, 2], P(('sp', 'tp')), may hold values from 0 to 15, all different within a row; in each aligned block of 32 rows (0 to 31, 32 to 63, ...) at most 6 rows name the same one
- route_weights: float32 [8192, 2], P(('sp', 'tp')), may hold values from 0.2 to 1
- expert_gate: bfloat16 [16, 2048, 6144], P('sp', None, 'tp'), may hold values from -0.125 to 0.125
- expert_up: bfloat16 [16, 2048, 6144], P('sp', None, 'tp'), may hold values from -0.125 to 0.125
- expert_down: bfloat16 [16, 6144, 2048], P('sp', 'tp'), may hold values from -0.078125 to 0.078125
Outputs:
- out: bfloat16 [8192, 2048], P(('sp', 'tp'))
The draws below stay inside these ranges and needn't reach their ends.
Inputs may be any that keep to these rules, and one draw needn't show every extreme that they name: `route_ids`: each row names 2 different experts. Within the rows of one device (aligned blocks of 32 rows) no expert is named by more than 6 rows, and in every draw some device's block names some expert exactly 6 times.
All inputs are finite; a program needn't handle non-finite values.
Results may differ from the reference program's by a relative error of at most 0.02.
Values may be sent and summed in bfloat16 or wider, within the bound.
A program may use at most 128 MiB of HBM per device.

```python
import math
import jax
import jax.numpy as jnp
import numpy as np
from jax import lax

D = 2048
HEADS_A = 16
QK_A = 64
V_A = 128
HEADS_B = 16
QK_B = 32
V_B = 64
FF = 6144
TOP = 2
SEQ_DEV = 512
EXPERTS = 16
TOK_DEV = 32
CAP = 6
TOKENS = 8192
N_TP = 16


def drawn_pair(key, heads, width):
    shape = (TOKENS, heads, 2 * width)
    query = jnp.clip(jax.random.normal(jax.random.fold_in(key, 21), shape, jnp.float32) * 1.3, -8.0, 8.0)
    keys = jnp.clip(jax.random.normal(jax.random.fold_in(key, 22), shape, jnp.float32) * 1.3, -8.0, 8.0)
    return (query, keys)


def draw_query_a(key, part):
    return drawn_pair(jax.random.fold_in(key, 1), HEADS_A, QK_A)[0].astype(jnp.bfloat16)


def draw_key_a(key, part):
    return drawn_pair(jax.random.fold_in(key, 1), HEADS_A, QK_A)[1].astype(jnp.bfloat16)


def draw_query_b(key, part):
    return drawn_pair(jax.random.fold_in(key, 2), HEADS_B, QK_B)[0].astype(jnp.bfloat16)


def draw_key_b(key, part):
    return drawn_pair(jax.random.fold_in(key, 2), HEADS_B, QK_B)[1].astype(jnp.bfloat16)


def level_of(stream_key, shape, split, smallest, largest):
    def one(axis_at, parts):
        steps = jax.random.uniform(jax.random.fold_in(jax.random.fold_in(stream_key, 6), axis_at), (parts,), jnp.float32, smallest / len(split), largest / len(split))
        return jnp.repeat(jnp.exp(steps), shape[axis_at] // parts).reshape((-1,) + (1,) * (len(shape) - axis_at - 1))

    loudness = one(*split[0])
    for cut in split[1:]:
        loudness = loudness * one(*cut)
    return loudness


def routed_block(key, own, number, rows, number_of, top, most, skew):
    order = jax.random.permutation(key, number_of)
    packed, common = shares(number_of, rows * top, most, skew, True), shares(number_of, rows * top, most, skew, False)
    places = jnp.arange(number_of)

    def named(tallies, turn):
        used = int((tallies > 0).sum())
        fixed = max(1, used // 4)
        moved = fixed + (places - fixed + turn * (used - fixed)) % max(1, number_of - fixed)
        return jnp.zeros((number_of,), jnp.int32).at[order[jnp.where(places < fixed, places, moved)]].set(jnp.asarray(tallies, jnp.int32))

    tallies = jnp.where(number % 4 == 0, named(packed, number // 4), named(common, number - number // 4 - 1))
    mixed = jax.random.permutation(jax.random.fold_in(own, 3), number_of)
    source_of, sink = mixed[0:number_of // 2 * 2:2], mixed[1:number_of // 2 * 2:2]
    margin = jnp.minimum(tallies[source_of] - 1, most - tallies[sink]) // 2
    margin = jnp.where((source_of == order[0]) | (sink == order[0]) | (tallies[sink] == 0), 0, jnp.maximum(margin, 0))
    moved = jax.random.randint(jax.random.fold_in(own, 4), (number_of // 2,), 0, 1 << 20) % (margin + 1)
    tallies = tallies.at[source_of].add(-moved).at[sink].add(moved)
    items = jnp.searchsorted(jnp.cumsum(tallies), jnp.arange(rows * top), side="right").astype(jnp.int32)
    table = items.reshape(top, rows).T
    table = table[jax.random.permutation(jax.random.fold_in(own, 1), rows)]
    turn = jax.random.randint(jax.random.fold_in(own, 2), (rows, 1), 0, top)
    return jnp.take_along_axis(table, (jnp.arange(top)[None, :] + turn) % top, axis=1)


def shares(number_of, total, reach, skew, full):
    loads = [(1 << 20) // math.isqrt(grade ** skew) + 1 for grade in range(1, number_of + 1)]
    largest = reach if full else min(reach, max(-(-total // number_of), total * loads[0] // sum(loads)))
    least = 1 if total - largest >= number_of - 1 else 0
    given, spare = [largest] + [least] * (number_of - 1), total - largest - least * (number_of - 1)
    while spare > 0:
        movable = [i for i in range(1, number_of) if given[i] < largest] or [i for i in range(1, number_of) if given[i] < reach]
        mass, remaining = sum([loads[i] for i in movable]), spare
        for i in movable:
            more = min(reach - given[i], max(1, remaining * loads[i] // mass), spare)
            given[i] = given[i] + more
            spare = spare - more
    return np.array(given)


def gaussian(stream_key, dims, scale, most, shards=(), held_as=jnp.bfloat16):
    drawn = jax.random.normal(stream_key, dims, jnp.float32) * scale
    if len(shards) > 0:
        drawn = level_of(stream_key, dims, shards, -0.22, 0.18) * drawn
    return jnp.clip(drawn, min=-most, max=most).astype(held_as)


def setup_inputs(seed: int = 0) -> dict:
    streams_of = jax.random.split(jax.random.key(seed), 20)
    resid = gaussian(streams_of[0], (TOKENS, D), 1.0, 6.0, ((0, 256),))
    query_a = draw_query_a(jax.random.fold_in(streams_of[19], 71), 0)
    key_a = draw_key_a(jax.random.fold_in(streams_of[19], 71), 0)
    value_a = gaussian(streams_of[3], (TOKENS, HEADS_A, V_A), 1.0, 6.0, ((0, 16), (1, 16)))
    query_b = draw_query_b(jax.random.fold_in(streams_of[19], 71), 0)
    key_b = draw_key_b(jax.random.fold_in(streams_of[19], 71), 0)
    value_b = gaussian(streams_of[6], (TOKENS, HEADS_B, V_B), 1.0, 6.0, ((0, 16), (1, 16)))
    mix_a = jnp.clip(0.3 + 0.5 * jax.random.uniform(streams_of[7], (HEADS_A,), jnp.float32) ** level_of(streams_of[7], (HEADS_A,), ((0, 16),), -0.2, 0.2), 0.3, 0.8)
    mix_b = jnp.clip(0.3 + 0.5 * jax.random.uniform(streams_of[8], (HEADS_B,), jnp.float32) ** level_of(streams_of[8], (HEADS_B,), ((0, 16),), -0.2, 0.2), 0.3, 0.8)
    head_gain_a = jnp.clip(1.0 + 0.18 * jax.random.normal(streams_of[9], (V_A,), jnp.float32), 0.1, 1.9)
    head_gain_b = jnp.clip(1.0 + 0.18 * jax.random.normal(streams_of[10], (V_B,), jnp.float32), 0.1, 1.9)
    proj_a = gaussian(streams_of[11], (HEADS_A * V_A, D), (HEADS_A * V_A + HEADS_B * V_B) ** -0.5, 0.109375, ((0, 16),))
    proj_b = gaussian(streams_of[12], (HEADS_B * V_B, D), (HEADS_A * V_A + HEADS_B * V_B) ** -0.5, 0.109375, ((0, 16),))
    norm_gain = jnp.clip(1.0 + 0.18 * jax.random.normal(streams_of[13], (D,), jnp.float32), 0.1, 1.9)
    route_ids_keys = jax.random.split(jax.random.fold_in(streams_of[14], 1), TOKENS // TOK_DEV)
    route_ids_turns = jax.random.permutation(jax.random.fold_in(streams_of[14], 3), TOKENS // TOK_DEV)
    route_ids = jax.vmap(lambda own, number: routed_block(jax.random.fold_in(streams_of[14], 2), own, number, TOK_DEV, EXPERTS, TOP, CAP, 1))(route_ids_keys, route_ids_turns).reshape((TOKENS, TOP))
    route_weights = jnp.clip(0.2 + 0.8 * jax.random.uniform(streams_of[15], (TOKENS, TOP), jnp.float32) ** level_of(streams_of[15], (TOKENS, TOP), ((0, 256),), -0.2, 0.2), 0.2, 1.0)
    expert_gate = gaussian(streams_of[16], (EXPERTS, D, FF), D ** -0.5, 0.125, ((0, 16), (2, 16)))
    expert_up = gaussian(streams_of[17], (EXPERTS, D, FF), D ** -0.5, 0.125, ((0, 16), (2, 16)))
    expert_down = gaussian(streams_of[18], (EXPERTS, FF, D), FF ** -0.5, 0.078125, ((0, 16), (1, 16)))
    return {"resid": resid, "query_a": query_a, "key_a": key_a, "value_a": value_a, "query_b": query_b, "key_b": key_b, "value_b": value_b, "mix_a": mix_a, "mix_b": mix_b, "head_gain_a": head_gain_a, "head_gain_b": head_gain_b, "proj_a": proj_a, "proj_b": proj_b, "norm_gain": norm_gain, "route_ids": route_ids, "route_weights": route_weights, "expert_gate": expert_gate, "expert_up": expert_up, "expert_down": expert_down}


EPS = 1e-06
HEAD_SCALE = 1.0 - (0.8 - 0.6 * math.exp(-0.3))

def attend(query, key, value, mix, gain):
    length, heads, double = query.shape
    width = double // 2
    scale = 1.0 / math.sqrt(width)
    block_rows = SEQ_DEV // 2
    keys_float = key.astype(jnp.float32)
    values_float = value.astype(jnp.float32)
    key_pos = jnp.arange(length, dtype=jnp.int32)

    def one_block(index):
        first = index * block_rows
        block = lax.dynamic_slice_in_dim(query, first, block_rows, 0).astype(jnp.float32)
        query_pos = first + jnp.arange(block_rows, dtype=jnp.int32)
        allowed = key_pos[None, :] <= query_pos[:, None]
        results = []
        for which in range(2):
            scores = jnp.einsum('qhd,khd->hqk', block[:, :, which * width:(which + 1) * width], keys_float[:, :, which * width:(which + 1) * width]) * scale
            scores = jnp.where(allowed[None], scores, -jnp.inf)
            shifted = jnp.exp(scores - lax.optimization_barrier(jnp.max(scores, axis=2, keepdims=True)))
            sums = lax.optimization_barrier(jnp.sum(shifted, axis=2))
            rounded = lax.optimization_barrier(shifted.astype(jnp.bfloat16)).astype(jnp.float32)
            weighted = jnp.einsum('hqk,khv->qhv', rounded, values_float)
            results.append(weighted / jnp.transpose(sums)[:, :, None])
        return results[0] - mix[None, :, None] * results[1]
    mixed = lax.map(one_block, jnp.arange(length // block_rows, dtype=jnp.int32))
    mixed = mixed.reshape(length, heads, -1)
    normed = mixed * lax.rsqrt(lax.optimization_barrier(jnp.mean(mixed * mixed, axis=2, keepdims=True)) + EPS) * gain * HEAD_SCALE
    return normed.astype(jnp.bfloat16).reshape(length, -1)

def slot_numbers(route_rows, experts, capacity):
    count, top_count = route_rows.shape
    flat = route_rows.reshape(count * top_count)
    onehot = (flat[:, None] == jnp.arange(experts, dtype=jnp.int32)[None, :]).astype(jnp.int32)
    ranks = lax.optimization_barrier(jnp.sum((jnp.cumsum(onehot, axis=0) - onehot) * onehot, axis=1))
    return (flat * capacity + ranks).reshape(count, top_count)

def reference(resid, query_a, key_a, value_a, query_b, key_b, value_b, mix_a, mix_b, head_gain_a, head_gain_b, proj_a, proj_b, norm_gain, route_ids, route_weights, expert_gate, expert_up, expert_down):
    heads_a = attend(query_a, key_a, value_a, mix_a, head_gain_a)
    heads_b = attend(query_b, key_b, value_b, mix_b, head_gain_b)
    cols_a = heads_a.shape[1] // N_TP
    cols_b = heads_b.shape[1] // N_TP
    mixed = resid.astype(jnp.float32)
    for shard in range(N_TP):
        partial_sum = jnp.dot(heads_a[:, shard * cols_a:(shard + 1) * cols_a], proj_a[shard * cols_a:(shard + 1) * cols_a], preferred_element_type=jnp.float32)
        partial_sum = partial_sum + jnp.dot(heads_b[:, shard * cols_b:(shard + 1) * cols_b], proj_b[shard * cols_b:(shard + 1) * cols_b], preferred_element_type=jnp.float32)
        mixed = mixed + lax.optimization_barrier(partial_sum.astype(jnp.bfloat16)).astype(jnp.float32)
    normed = (mixed * lax.rsqrt(lax.optimization_barrier(jnp.mean(mixed * mixed, axis=1, keepdims=True)) + EPS) * norm_gain).astype(jnp.bfloat16)
    blocks = TOKENS // TOK_DEV
    local = jax.vmap(lambda rows_in: slot_numbers(rows_in, EXPERTS, CAP))(route_ids.reshape(blocks, TOK_DEV, TOP))
    row_index = (jnp.arange(blocks, dtype=jnp.int32)[:, None, None] * CAP + local % CAP).reshape(-1)
    expert_index = route_ids.reshape(-1)
    buffer = jnp.zeros((EXPERTS, blocks * CAP, D), jnp.bfloat16)
    buffer = buffer.at[expert_index, row_index].set(jnp.repeat(normed, TOP, axis=0))
    block_width = FF // N_TP

    def run_expert(operands):
        rows_in, gate_w, up_w, down_w = operands
        gate = jnp.dot(rows_in, gate_w, preferred_element_type=jnp.float32)
        upward = jnp.dot(rows_in, up_w, preferred_element_type=jnp.float32)
        hidden = (jax.nn.silu(gate) * upward).astype(jnp.bfloat16)
        summed = jnp.zeros((rows_in.shape[0], D), jnp.float32)
        for shard in range(N_TP):
            part = jnp.dot(hidden[:, shard * block_width:(shard + 1) * block_width], down_w[shard * block_width:(shard + 1) * block_width], preferred_element_type=jnp.float32)
            summed = summed + lax.optimization_barrier(part.astype(jnp.bfloat16)).astype(jnp.float32)
        return summed.astype(jnp.bfloat16)
    outputs = lax.map(run_expert, (buffer, expert_gate, expert_up, expert_down))
    picked = outputs[expert_index, row_index].reshape(TOKENS, TOP, D).astype(jnp.float32)
    result = mixed + lax.optimization_barrier(jnp.sum(route_weights[:, :, None] * picked, axis=1))
    return result.astype(jnp.bfloat16)
```

```python
import math

import jax
import jax.numpy as jnp
from jax import lax
from jax.experimental import pallas as pl
from jax.experimental.pallas import tpu as pltpu
from jax.sharding import PartitionSpec as P

EPS = 1e-06
NEG = -1e30
HEAD_SCALE = 1.0 - (0.8 - 0.6 * math.exp(-0.3))


def cut_along(value, dim, size):
    before, after = (value.shape[:dim], value.shape[dim + 1 :])
    return jnp.moveaxis(value.reshape(*before, size, -1, *after), dim, 0)


def sent_and_summed(value, axis, dim):
    parts = cut_along(value, dim, lax.axis_size(axis))
    arrived = lax.all_to_all(parts, axis, split_axis=0, concat_axis=0, tiled=True)
    return arrived.astype(jnp.float32).sum(axis=0)


def rms_scaled(values, gain):
    return values * lax.rsqrt(jnp.mean(values * values, axis=-1, keepdims=True) + EPS) * gain


def slot_numbers(route_rows, experts, capacity):
    count, top_count = route_rows.shape
    flat = route_rows.reshape(count * top_count)
    onehot = (flat[:, None] == jnp.arange(experts, dtype=jnp.int32)[None, :]).astype(jnp.int32)
    ranks = jnp.sum((jnp.cumsum(onehot, axis=0) - onehot) * onehot, axis=1)
    return (flat * capacity + ranks).reshape(count, top_count)


MESH = pl.DeviceIdType.MESH
LOG2E = 1.4426950408889634
PART = 128


def dot32(a, b):
    return jnp.dot(a, b, preferred_element_type=jnp.float32)


def attention_kernel(
    qa_ref, qb_ref, ka_ref, va_ref, kb_ref, vb_ref, mix_ref, gain_a_ref, gain_b_ref,
    out_ref,
    buf, qta, qtb, acc_a, acc_b, m_ref, l_ref, send_sem, recv_sem,
):
    place = lax.axis_index("sp")
    tp = lax.axis_index("tp")
    y, x = place // 4, place % 4
    half = buf.shape[2]

    def at(ox, oy):
        return ((y + oy + 4) % 4) * 4 + (x + ox + 4) % 4

    def spot(h, df, dg):
        return at(df, dg) if h == 0 else at(dg, df)

    barrier = pltpu.get_barrier_semaphore()
    for ox, oy in ((1, 0), (-1, 0), (0, 1), (0, -1)):
        pl.semaphore_signal(barrier, inc=1, device_id=(at(ox, oy), tp), device_id_type=MESH)

    va_t = jnp.transpose(va_ref[...])
    for h in range(2):
        cols = slice(h * half, (h + 1) * half)
        buf[place, h, :, 0:128] = ka_ref[cols, :]
        buf[place, h, 0:128, 128:384] = va_t[:, cols]
        buf[place, h, 128:192, 128:384] = kb_ref[:, cols]
        buf[place, h, 192:256, 128:384] = vb_ref[:, cols]

    pl.semaphore_wait(barrier, 4)

    def region(h, df, dg, part):
        ref = buf.at[spot(h, df, dg), h]
        return ref if part is None else ref.at[pl.ds(part * PART, PART)]

    def copy(h, number, df, dg, part, to_f, to_g):
        ref = region(h, df, dg, part)
        return pltpu.make_async_remote_copy(
            src_ref=ref,
            dst_ref=ref,
            send_sem=send_sem.at[h * 20 + number],
            recv_sem=recv_sem.at[h * 20 + number],
            device_id=(spot(h, to_f, to_g), tp),
            device_id_type=MESH,
        )

    moves = {
        0: (0, 0, None, 1, 0), 1: (0, 0, None, -1, 0),
        2: (0, 0, None, 0, 1), 3: (0, 0, None, 0, -1),
        4: (-1, 0, 0, 1, 0), 5: (1, 0, 1, -1, 0),
        6: (-1, 0, None, 0, 1), 7: (-1, 0, None, 0, -1),
        8: (1, 0, None, 0, 1), 9: (1, 0, None, 0, -1),
        10: (2, 0, None, 0, 1), 11: (2, 0, None, 0, -1),
        12: (0, -1, 0, 0, 1), 13: (0, 1, 1, 0, -1),
        14: (-1, -1, 0, 0, 1), 15: (-1, 1, 1, 0, -1),
        16: (1, -1, 0, 0, 1), 17: (1, 1, 1, 0, -1),
        18: (2, -1, 0, 0, 1), 19: (2, 1, 1, 0, -1),
    }

    def start(*numbers):
        for number in numbers:
            for h in range(2):
                copy(h, number, *moves[number]).start()

    def arrive(number, *then):
        df, dg, part, to_f, to_g = moves[number]
        for h in range(2):
            copy(h, number, df - to_f, dg - to_g, part, to_f, to_g).wait_recv()
            for follow in then:
                copy(h, follow, *moves[follow]).start()

    start(0, 1, 2, 3)

    qa_t = jnp.transpose(qa_ref[...])
    zero_a = jnp.zeros((64, half), jnp.bfloat16)
    zero_b = jnp.zeros((32, half), jnp.bfloat16)
    for h in range(2):
        cols = slice(h * half, (h + 1) * half)
        qta[h, 0:64, :] = qa_t[0:64, cols]
        qta[h, 64:128, :] = zero_a
        qta[2 + h, 0:64, :] = zero_a
        qta[2 + h, 64:128, :] = qa_t[64:128, cols]
        qtb[h, 0:32, :] = qb_ref[0:32, cols]
        qtb[h, 32:64, :] = zero_b
        qtb[2 + h, 0:32, :] = zero_b
        qtb[2 + h, 32:64, :] = qb_ref[32:64, cols]
    acc_a[...] = jnp.zeros_like(acc_a)
    acc_b[...] = jnp.zeros_like(acc_b)
    m_ref[...] = jnp.full_like(m_ref, NEG)
    l_ref[...] = jnp.zeros_like(l_ref)

    def fold(index, slot, scores, v_parts, acc, factor, offsets):
        if offsets is not None:
            query_pos = lax.rem(index, 2) * half + lax.broadcasted_iota(jnp.int32, (half, half), 1)
            scores = [
                jnp.where(
                    lax.broadcasted_iota(jnp.int32, (half, half), 0) + first <= query_pos, s, NEG
                )
                for s, first in zip(scores, offsets)
            ]
        top = jnp.maximum(
            jnp.max(scores[0], axis=0, keepdims=True), jnp.max(scores[1], axis=0, keepdims=True)
        )
        old = m_ref[slot]
        fresh = jnp.maximum(old, top)
        scale = jnp.exp2((old - fresh) * factor)
        weights = [jnp.exp2((s - fresh) * factor) for s in scores]
        m_ref[slot] = fresh
        l_ref[slot] = (
            l_ref[slot] * scale
            + jnp.sum(weights[0], axis=0, keepdims=True)
            + jnp.sum(weights[1], axis=0, keepdims=True)
        )
        acc[index] = (
            acc[index] * scale
            + dot32(v_parts[0], weights[0].astype(jnp.bfloat16))
            + dot32(v_parts[1], weights[1].astype(jnp.bfloat16))
        )

    def block(source, offsets):
        k_b = [jnp.transpose(buf[source, h, 128:192, 128:384]) for h in range(2)]

        def tile(index, carry):
            q_a, q_b = qta[index], qtb[index]
            fold(
                index, index,
                [dot32(buf[source, h, :, 0:128], q_a) for h in range(2)],
                [buf[source, h, 0:128, 128:384] for h in range(2)],
                acc_a, LOG2E / 8.0, offsets,
            )
            fold(
                index, index + 4,
                [dot32(k_b[h], q_b) for h in range(2)],
                [buf[source, h, 192:256, 128:384] for h in range(2)],
                acc_b, LOG2E / math.sqrt(32.0), offsets,
            )
            return carry

        lax.fori_loop(0, 4, tile, 0)

    def group(offsets):
        def step(number, carry):
            ox, oy = jnp.int32(0), jnp.int32(0)
            for which, (dx, dy) in enumerate(offsets):
                ox = jnp.where(number == which, dx, ox)
                oy = jnp.where(number == which, dy, oy)
            source = at(ox, oy)

            @pl.when(source < place)
            def _():
                block(source, None)

            return carry

        lax.fori_loop(0, len(offsets), step, 0)

    block(place, (0, half))
    arrive(0, 4, 6, 7)
    arrive(1, 5, 8, 9)
    arrive(2, 12)
    arrive(3, 13)
    group(((-1, 0), (0, -1), (1, 0), (0, 1)))
    arrive(4)
    arrive(5, 10, 11)
    arrive(6, 14)
    arrive(7, 15)
    arrive(8, 16)
    arrive(9, 17)
    arrive(12)
    arrive(13)
    group(((-1, -1), (1, -1), (-1, 1), (1, 1), (2, 0), (0, 2)))
    arrive(10, 18)
    arrive(11, 19)
    for number in (14, 15, 16, 17):
        arrive(number)
    group(((2, -1), (-1, 2), (1, 2), (2, 1)))
    arrive(18)
    arrive(19)
    group(((2, 2),))

    for h in range(2):
        for acc, base, which, gain, first in (
            (acc_a, 0, 0, gain_a_ref, 0), (acc_b, 4, 1, gain_b_ref, 128),
        ):
            one = acc[h] / l_ref[base + h]
            two = acc[2 + h] / l_ref[base + 2 + h]
            mixed = one - mix_ref[which] * two
            mixed = mixed * lax.rsqrt(jnp.mean(mixed * mixed, axis=0, keepdims=True) + EPS)
            rows = jnp.transpose(mixed) * gain[...] * HEAD_SCALE
            out_ref[h * half : (h + 1) * half, first : first + rows.shape[1]] = rows.astype(
                jnp.bfloat16
            )
    for number in range(20):
        for h in range(2):
            copy(h, number, *moves[number]).wait_send()


def attention(query_a, key_a, value_a, query_b, key_b, value_b, mix_a, mix_b, gain_a, gain_b):
    rows = query_a.shape[0]
    vmem = pl.BlockSpec(memory_space=pltpu.VMEM)
    return pl.pallas_call(
        attention_kernel,
        out_shape=jax.ShapeDtypeStruct((rows, 192), jnp.bfloat16),
        in_specs=[vmem] * 6 + [pl.BlockSpec(memory_space=pltpu.SMEM)] + [vmem] * 2,
        out_specs=vmem,
        scratch_shapes=[
            pltpu.VMEM((16, 2, 256, 384), jnp.bfloat16),
            pltpu.VMEM((4, 128, 256), jnp.bfloat16),
            pltpu.VMEM((4, 64, 256), jnp.bfloat16),
            pltpu.VMEM((4, 128, 256), jnp.float32),
            pltpu.VMEM((4, 64, 256), jnp.float32),
            pltpu.VMEM((8, 1, 256), jnp.float32),
            pltpu.VMEM((8, 1, 256), jnp.float32),
            pltpu.SemaphoreType.DMA((40,)),
            pltpu.SemaphoreType.DMA((40,)),
        ],
        compiler_params=pltpu.CompilerParams(collective_id=0, has_side_effects=True),
    )(
        query_a[:, 0, :], query_b[:, 0, :].T, key_a[:, 0, :], value_a[:, 0, :],
        key_b[:, 0, :].T, value_b[:, 0, :].T,
        jnp.concatenate([mix_a, mix_b]), gain_a[None, :], gain_b[None, :],
    )


def per_device(
    resid,
    query_a,
    key_a,
    value_a,
    query_b,
    key_b,
    value_b,
    mix_a,
    mix_b,
    head_gain_a,
    head_gain_b,
    proj_a,
    proj_b,
    norm_gain,
    route_ids,
    route_weights,
    expert_gate,
    expert_up,
    expert_down,
):
    sp_ways = lax.axis_size("sp")
    heads_out = attention(
        query_a, key_a, value_a, query_b, key_b, value_b, mix_a, mix_b, head_gain_a, head_gain_b
    )
    width = resid.shape[1]
    tok_rows = resid.shape[0]
    top_count = route_ids.shape[1]
    capacity = 3 * top_count * tok_rows // (2 * sp_ways)
    own_slots = slot_numbers(route_ids, sp_ways, capacity)
    term = jnp.dot(heads_out[:, :128], proj_a, preferred_element_type=jnp.float32)
    term = term + jnp.dot(heads_out[:, 128:], proj_b, preferred_element_type=jnp.float32)
    mixed = resid.astype(jnp.float32) + sent_and_summed(
        lax.optimization_barrier(term.astype(jnp.bfloat16))
        .astype(jnp.float32)
        .astype(jnp.bfloat16),
        "tp",
        0,
    )
    normed = rms_scaled(mixed, norm_gain).astype(jnp.bfloat16)
    lookup = jnp.arange(sp_ways * capacity, dtype=jnp.int32)[:, None]
    spread = jnp.zeros((sp_ways * capacity, tok_rows), jnp.float32)
    for which in range(top_count):
        spread = spread + (own_slots[:, which][None, :] == lookup).astype(jnp.float32)
    outgoing = jnp.dot(
        spread.astype(jnp.bfloat16), normed, preferred_element_type=jnp.float32
    ).astype(jnp.bfloat16)
    arrived = lax.all_to_all(
        outgoing.reshape(sp_ways, capacity, width), "sp", split_axis=0, concat_axis=0, tiled=True
    )
    piece = lax.all_gather(arrived.reshape(sp_ways * capacity, width), "tp", axis=0, tiled=True)
    gate = jnp.dot(piece, expert_gate[0], preferred_element_type=jnp.float32)
    upward = jnp.dot(piece, expert_up[0], preferred_element_type=jnp.float32)
    hidden = (jax.nn.silu(gate) * upward).astype(jnp.bfloat16)
    term = jnp.dot(hidden, expert_down[0], preferred_element_type=jnp.float32)
    summed = lax.psum_scatter(
        lax.optimization_barrier(term.astype(jnp.bfloat16))
        .astype(jnp.float32)
        .astype(jnp.bfloat16),
        "tp",
        scatter_dimension=0,
        tiled=True,
    )
    finished_rows = summed.reshape(sp_ways, capacity, width)
    back = lax.all_to_all(finished_rows, "sp", split_axis=0, concat_axis=0, tiled=True)
    picked = jnp.take(back.reshape(sp_ways * capacity, width), own_slots.reshape(-1), axis=0)
    picked = picked.reshape(tok_rows, top_count, width)
    output = mixed + jnp.sum(route_weights[:, :, None] * picked.astype(jnp.float32), axis=1)
    return output.astype(jnp.bfloat16)


def solution(mesh):
    placed = (
        P(("sp", "tp"), None),
        P("sp", "tp", None),
        P("sp", "tp", None),
        P("sp", "tp", None),
        P("sp", "tp", None),
        P("sp", "tp", None),
        P("sp", "tp", None),
        P("tp"),
        P("tp"),
        P(),
        P(),
        P("tp", None),
        P("tp", None),
        P(),
        P(("sp", "tp"), None),
        P(("sp", "tp"), None),
        P("sp", None, "tp"),
        P("sp", None, "tp"),
        P("sp", "tp", None),
    )
    return jax.shard_map(
        per_device, mesh=mesh, in_specs=placed, out_specs=P(("sp", "tp"), None), check_vma=False
    )
```

```python
import math

import jax
import jax.numpy as jnp
from jax import lax
from jax.experimental import pallas as pl
from jax.experimental.pallas import tpu as pltpu
from jax.sharding import PartitionSpec as P

EPS = 1e-06
NEG = -1e30
HEAD_SCALE = 1.0 - (0.8 - 0.6 * math.exp(-0.3))


def rms_scaled(values, gain):
    return values * lax.rsqrt(jnp.mean(values * values, axis=-1, keepdims=True) + EPS) * gain


def slot_numbers(route_rows, experts, capacity):
    count, top_count = route_rows.shape
    flat = route_rows.reshape(count * top_count)
    onehot = (flat[:, None] == jnp.arange(experts, dtype=jnp.int32)[None, :]).astype(jnp.int32)
    ranks = jnp.sum((jnp.cumsum(onehot, axis=0) - onehot) * onehot, axis=1)
    return (flat * capacity + ranks).reshape(count, top_count)


MESH = pl.DeviceIdType.MESH
LOG2E = 1.4426950408889634
PART = 128


def dot32(a, b):
    return jnp.dot(a, b, preferred_element_type=jnp.float32)


def attention_kernel(
    qa_ref, qb_ref, ka_ref, va_ref, kb_ref, vb_ref, mix_ref, gain_a_ref, gain_b_ref,
    out_ref,
    buf, qta, qtb, acc_a, acc_b, m_ref, l_ref, send_sem, recv_sem,
):
    place = lax.axis_index("sp")
    tp = lax.axis_index("tp")
    y, x = place // 4, place % 4
    half = buf.shape[2]

    def at(ox, oy):
        return ((y + oy + 4) % 4) * 4 + (x + ox + 4) % 4

    def spot(h, df, dg):
        return at(df, dg) if h == 0 else at(dg, df)

    barrier = pltpu.get_barrier_semaphore()
    for ox, oy in ((1, 0), (-1, 0), (0, 1), (0, -1)):
        pl.semaphore_signal(barrier, inc=1, device_id=(at(ox, oy), tp), device_id_type=MESH)

    va_t = jnp.transpose(va_ref[...])
    for h in range(2):
        cols = slice(h * half, (h + 1) * half)
        buf[place, h, :, 0:128] = ka_ref[cols, :]
        buf[place, h, 0:128, 128:384] = va_t[:, cols]
        buf[place, h, 128:192, 128:384] = kb_ref[:, cols]
        buf[place, h, 192:256, 128:384] = vb_ref[:, cols]

    pl.semaphore_wait(barrier, 4)

    def region(h, df, dg, part):
        ref = buf.at[spot(h, df, dg), h]
        return ref if part is None else ref.at[pl.ds(part * PART, PART)]

    def copy(h, number, df, dg, part, to_f, to_g):
        ref = region(h, df, dg, part)
        return pltpu.make_async_remote_copy(
            src_ref=ref,
            dst_ref=ref,
            send_sem=send_sem.at[h * 20 + number],
            recv_sem=recv_sem.at[h * 20 + number],
            device_id=(spot(h, to_f, to_g), tp),
            device_id_type=MESH,
        )

    moves = {
        0: (0, 0, None, 1, 0), 1: (0, 0, None, -1, 0),
        2: (0, 0, None, 0, 1), 3: (0, 0, None, 0, -1),
        4: (-1, 0, 0, 1, 0), 5: (1, 0, 1, -1, 0),
        6: (-1, 0, None, 0, 1), 7: (-1, 0, None, 0, -1),
        8: (1, 0, None, 0, 1), 9: (1, 0, None, 0, -1),
        10: (2, 0, None, 0, 1), 11: (2, 0, None, 0, -1),
        12: (0, -1, 0, 0, 1), 13: (0, 1, 1, 0, -1),
        14: (-1, -1, 0, 0, 1), 15: (-1, 1, 1, 0, -1),
        16: (1, -1, 0, 0, 1), 17: (1, 1, 1, 0, -1),
        18: (2, -1, 0, 0, 1), 19: (2, 1, 1, 0, -1),
    }

    def start(*numbers):
        for number in numbers:
            for h in range(2):
                copy(h, number, *moves[number]).start()

    def arrive(number, *then):
        df, dg, part, to_f, to_g = moves[number]
        for h in range(2):
            copy(h, number, df - to_f, dg - to_g, part, to_f, to_g).wait_recv()
            for follow in then:
                copy(h, follow, *moves[follow]).start()

    start(0, 1, 2, 3)

    qa_t = jnp.transpose(qa_ref[...])
    zero_a = jnp.zeros((64, half), jnp.bfloat16)
    zero_b = jnp.zeros((32, half), jnp.bfloat16)
    for h in range(2):
        cols = slice(h * half, (h + 1) * half)
        qta[h, 0:64, :] = qa_t[0:64, cols]
        qta[h, 64:128, :] = zero_a
        qta[2 + h, 0:64, :] = zero_a
        qta[2 + h, 64:128, :] = qa_t[64:128, cols]
        qtb[h, 0:32, :] = qb_ref[0:32, cols]
        qtb[h, 32:64, :] = zero_b
        qtb[2 + h, 0:32, :] = zero_b
        qtb[2 + h, 32:64, :] = qb_ref[32:64, cols]
    acc_a[...] = jnp.zeros_like(acc_a)
    acc_b[...] = jnp.zeros_like(acc_b)
    m_ref[...] = jnp.full_like(m_ref, NEG)
    l_ref[...] = jnp.zeros_like(l_ref)

    def fold(index, slot, scores, v_parts, acc, factor, offsets):
        if offsets is not None:
            query_pos = lax.rem(index, 2) * half + lax.broadcasted_iota(jnp.int32, (half, half), 1)
            scores = [
                jnp.where(
                    lax.broadcasted_iota(jnp.int32, (half, half), 0) + first <= query_pos, s, NEG
                )
                for s, first in zip(scores, offsets)
            ]
        top = jnp.maximum(
            jnp.max(scores[0], axis=0, keepdims=True), jnp.max(scores[1], axis=0, keepdims=True)
        )
        old = m_ref[slot]
        fresh = jnp.maximum(old, top)
        scale = jnp.exp2((old - fresh) * factor)
        weights = [jnp.exp2((s - fresh) * factor) for s in scores]
        m_ref[slot] = fresh
        l_ref[slot] = (
            l_ref[slot] * scale
            + jnp.sum(weights[0], axis=0, keepdims=True)
            + jnp.sum(weights[1], axis=0, keepdims=True)
        )
        acc[index] = (
            acc[index] * scale
            + dot32(v_parts[0], weights[0].astype(jnp.bfloat16))
            + dot32(v_parts[1], weights[1].astype(jnp.bfloat16))
        )

    def block(source, offsets):
        k_b = [jnp.transpose(buf[source, h, 128:192, 128:384]) for h in range(2)]

        def tile(index, carry):
            q_a, q_b = qta[index], qtb[index]
            fold(
                index, index,
                [dot32(buf[source, h, :, 0:128], q_a) for h in range(2)],
                [buf[source, h, 0:128, 128:384] for h in range(2)],
                acc_a, LOG2E / 8.0, offsets,
            )
            fold(
                index, index + 4,
                [dot32(k_b[h], q_b) for h in range(2)],
                [buf[source, h, 192:256, 128:384] for h in range(2)],
                acc_b, LOG2E / math.sqrt(32.0), offsets,
            )
            return carry

        lax.fori_loop(0, 4, tile, 0)

    def group(offsets):
        def step(number, carry):
            ox, oy = jnp.int32(0), jnp.int32(0)
            for which, (dx, dy) in enumerate(offsets):
                ox = jnp.where(number == which, dx, ox)
                oy = jnp.where(number == which, dy, oy)
            source = at(ox, oy)

            @pl.when(source < place)
            def _():
                block(source, None)

            return carry

        lax.fori_loop(0, len(offsets), step, 0)

    block(place, (0, half))
    arrive(0, 4, 6, 7)
    arrive(1, 5, 8, 9)
    arrive(2, 12)
    arrive(3, 13)
    group(((-1, 0), (0, -1), (1, 0), (0, 1)))
    arrive(4)
    arrive(5, 10, 11)
    arrive(6, 14)
    arrive(7, 15)
    arrive(8, 16)
    arrive(9, 17)
    arrive(12)
    arrive(13)
    group(((-1, -1), (1, -1), (-1, 1), (1, 1), (2, 0), (0, 2)))
    arrive(10, 18)
    arrive(11, 19)
    for number in (14, 15, 16, 17):
        arrive(number)
    group(((2, -1), (-1, 2), (1, 2), (2, 1)))
    arrive(18)
    arrive(19)
    group(((2, 2),))

    for h in range(2):
        for acc, base, which, gain, first in (
            (acc_a, 0, 0, gain_a_ref, 0), (acc_b, 4, 1, gain_b_ref, 128),
        ):
            one = acc[h] / l_ref[base + h]
            two = acc[2 + h] / l_ref[base + 2 + h]
            mixed = one - mix_ref[which] * two
            mixed = mixed * lax.rsqrt(jnp.mean(mixed * mixed, axis=0, keepdims=True) + EPS)
            rows = jnp.transpose(mixed) * gain[...] * HEAD_SCALE
            out_ref[h * half : (h + 1) * half, first : first + rows.shape[1]] = rows.astype(
                jnp.bfloat16
            )
    for number in range(20):
        for h in range(2):
            copy(h, number, *moves[number]).wait_send()


def attention(query_a, key_a, value_a, query_b, key_b, value_b, mix_a, mix_b, gain_a, gain_b):
    rows = query_a.shape[0]
    vmem = pl.BlockSpec(memory_space=pltpu.VMEM)
    return pl.pallas_call(
        attention_kernel,
        out_shape=jax.ShapeDtypeStruct((rows, 192), jnp.bfloat16),
        in_specs=[vmem] * 6 + [pl.BlockSpec(memory_space=pltpu.SMEM)] + [vmem] * 2,
        out_specs=vmem,
        scratch_shapes=[
            pltpu.VMEM((16, 2, 256, 384), jnp.bfloat16),
            pltpu.VMEM((4, 128, 256), jnp.bfloat16),
            pltpu.VMEM((4, 64, 256), jnp.bfloat16),
            pltpu.VMEM((4, 128, 256), jnp.float32),
            pltpu.VMEM((4, 64, 256), jnp.float32),
            pltpu.VMEM((8, 1, 256), jnp.float32),
            pltpu.VMEM((8, 1, 256), jnp.float32),
            pltpu.SemaphoreType.DMA((40,)),
            pltpu.SemaphoreType.DMA((40,)),
        ],
        compiler_params=pltpu.CompilerParams(collective_id=0, has_side_effects=True),
    )(
        query_a[:, 0, :], query_b[:, 0, :].T, key_a[:, 0, :], value_a[:, 0, :],
        key_b[:, 0, :].T, value_b[:, 0, :].T,
        jnp.concatenate([mix_a, mix_b]), gain_a[None, :], gain_b[None, :],
    )


def tp_place():
    tp = lax.axis_index("tp")
    return lax.axis_index("sp"), tp // 2, tp % 2


def meet_tp(sp, z, core):
    barrier = pltpu.get_barrier_semaphore()
    for peer in (((z + 1) % 8) * 2 + core, ((z + 7) % 8) * 2 + core, z * 2 + 1 - core):
        pl.semaphore_signal(barrier, inc=1, device_id=(sp, peer), device_id_type=MESH)
    pl.semaphore_wait(barrier, 3)


class Exchange:
    def __init__(self, pbuf, other, stage, landed, pair_send, pair_recv, ring_send, ring_recv):
        self.sp, self.z, self.core = tp_place()
        self.pbuf, self.other, self.stage, self.landed = pbuf, other, stage, landed
        self.pair_sems, self.ring_sems = (pair_send, pair_recv), (ring_send, ring_recv)
        self.rows = pbuf.shape[1] // 2

    def chip(self, offset):
        return (self.z + offset + 8) % 8

    def pair_copy(self, offset):
        chip = self.chip(offset)
        return pltpu.make_async_remote_copy(
            src_ref=self.pbuf.at[chip * 2 + 1 - self.core],
            dst_ref=self.other.at[chip],
            send_sem=self.pair_sems[0].at[offset + 3],
            recv_sem=self.pair_sems[1].at[offset + 3],
            device_id=(self.sp, self.z * 2 + 1 - self.core),
            device_id_type=MESH,
        )

    def ring_copy(self, way, half, distance):
        number = way * 8 + half * 4 + distance - 1
        return pltpu.make_async_remote_copy(
            src_ref=self.stage.at[way, half, distance - 1],
            dst_ref=self.landed.at[way, half, distance - 1],
            send_sem=self.ring_sems[0].at[number],
            recv_sem=self.ring_sems[1].at[number],
            device_id=(self.sp, self.chip(1 - 2 * way) * 2 + self.core),
            device_id_type=MESH,
        )

    def mine(self, offset, half):
        chip = self.chip(offset)
        rows = slice(half * self.rows, (half + 1) * self.rows)
        own = self.pbuf[chip * 2 + self.core, rows, :].astype(jnp.float32)
        return own + self.other[chip, rows, :].astype(jnp.float32)

    def send(self, way, half, distance):
        offset = distance * (1 - 2 * way)
        total = self.mine(4 if distance == 4 else offset, half)
        if distance < (4 if half == way else 3):
            self.ring_copy(way, half, distance + 1).wait_recv()
            total = total + self.landed[way, half, distance].astype(jnp.float32)
        self.stage[way, half, distance - 1] = total.astype(jnp.bfloat16)
        self.ring_copy(way, half, distance).start()

    def last(self, half):
        total = self.mine(0, half)
        for way in range(2):
            self.ring_copy(way, half, 1).wait_recv()
            total = total + self.landed[way, half, 0].astype(jnp.float32)
        return total

    def finish(self):
        for offset in range(-3, 5):
            self.pair_copy(offset).wait_send()
        for way in range(2):
            for half in range(2):
                for distance in range(1, 5 if half == way else 4):
                    self.ring_copy(way, half, distance).wait_send()


def exchange_scratch(rows, width):
    return [
        pltpu.VMEM((16, rows, width), jnp.bfloat16),
        pltpu.VMEM((8, rows, width), jnp.bfloat16),
        pltpu.VMEM((2, 2, 4, rows // 2, width), jnp.bfloat16),
        pltpu.VMEM((2, 2, 4, rows // 2, width), jnp.bfloat16),
        pltpu.SemaphoreType.DMA((8,)),
        pltpu.SemaphoreType.DMA((8,)),
        pltpu.SemaphoreType.DMA((16,)),
        pltpu.SemaphoreType.DMA((16,)),
    ]


def project_kernel(
    heads_ref, proj_a_ref, proj_b_ref, resid_ref, gain_ref, spread_ref, mixed_ref, out_ref,
    pbuf, other, stage, landed, pair_send, pair_recv, ring_send, ring_recv,
):
    sp, z, core = tp_place()
    ex = Exchange(pbuf, other, stage, landed, pair_send, pair_recv, ring_send, ring_recv)
    for first in range(0, 2048, 512):
        cols = slice(first, first + 512)
        term = dot32(heads_ref[:, 0:128], proj_a_ref[:, cols])
        term = term + dot32(heads_ref[:, 128:192], proj_b_ref[:, cols])
        pbuf[:, :, cols] = term.astype(jnp.bfloat16).reshape(16, 32, 512)
    meet_tp(sp, z, core)
    order = (4, 3, -3, 2, -2, 1, -1, 0)
    for offset in order:
        ex.pair_copy(offset).start()
    ex.pair_copy(4).wait_recv()
    ex.send(0, 0, 4)
    ex.send(1, 1, 4)
    for distance in (3, 2, 1):
        ex.pair_copy(distance).wait_recv()
        ex.pair_copy(-distance).wait_recv()
        if distance == 3:
            ex.send(0, 1, 3)
            ex.send(1, 0, 3)
        ex.send(0, 0, distance)
        ex.send(1, 1, distance)
        if distance < 3:
            ex.send(0, 1, distance)
            ex.send(1, 0, distance)
    ex.pair_copy(0).wait_recv()
    for half in range(2):
        rows = slice(half * 16, half * 16 + 16)
        mixed_ref[rows, :] = resid_ref[rows, :].astype(jnp.float32) + ex.last(half)
    normed = rms_scaled(mixed_ref[...], gain_ref[...]).astype(jnp.bfloat16)
    out_ref[...] = dot32(spread_ref[...], normed).astype(jnp.bfloat16)
    ex.finish()


def project(heads_out, proj_a, proj_b, resid, norm_gain, spread):
    rows, width = resid.shape
    vmem = pl.BlockSpec(memory_space=pltpu.VMEM)
    return pl.pallas_call(
        project_kernel,
        out_shape=(
            jax.ShapeDtypeStruct((rows, width), jnp.float32),
            jax.ShapeDtypeStruct((spread.shape[0], width), jnp.bfloat16),
        ),
        in_specs=[vmem] * 6,
        out_specs=(vmem, vmem),
        scratch_shapes=exchange_scratch(rows, width),
        compiler_params=pltpu.CompilerParams(collective_id=1, has_side_effects=True),
    )(heads_out, proj_a, proj_b, resid, norm_gain[None, :], spread)


def expert_kernel(
    rows_ref, gate_hbm, up_hbm, down_hbm, out_ref,
    xbuf, gate, up, down, w_sem, ag_send, ag_recv, share_send, share_recv,
    pbuf, other, stage, landed, pair_send, pair_recv, ring_send, ring_recv,
):
    sp, z, core = tp_place()
    ex = Exchange(pbuf, other, stage, landed, pair_send, pair_recv, ring_send, ring_recv)
    loads = [
        pltpu.make_async_copy(src, dst, w_sem.at[i])
        for i, (src, dst) in enumerate(((gate_hbm, gate), (up_hbm, up), (down_hbm, down)))
    ]
    for load in loads:
        load.start()
    xbuf[z * 2 + core] = rows_ref[...]
    meet_tp(sp, z, core)
    part = rows_ref.shape[0] // 2

    def shard(offset, half):
        chip = ex.chip(offset)
        return xbuf.at[chip * 2 + core, pl.ds(half * part, part)]

    def ag_copy(way, half, distance, arriving=False):
        sign = 1 - 2 * way
        away = distance + 1 if arriving else distance
        offset = 4 if away == 4 else -sign * away
        here = rows_ref.at[pl.ds(half * part, part)] if away == 0 else shard(offset, half)
        number = way * 8 + half * 4 + distance
        return pltpu.make_async_remote_copy(
            src_ref=here,
            dst_ref=shard(offset, half),
            send_sem=ag_send.at[number],
            recv_sem=ag_recv.at[number],
            device_id=(sp, ex.chip(sign) * 2 + core),
            device_id_type=MESH,
        )

    def share_copy(offset, half, arriving=False):
        chip = ex.chip(offset)
        there = xbuf.at[chip * 2 + (1 - core if arriving else core), pl.ds(half * part, part)]
        here = there
        if offset == 0 and not arriving:
            here = rows_ref.at[pl.ds(half * part, part)]
        number = (offset + 3) * 2 + half
        return pltpu.make_async_remote_copy(
            src_ref=here,
            dst_ref=there,
            send_sem=share_send.at[number],
            recv_sem=share_recv.at[number],
            device_id=(sp, z * 2 + 1 - core),
            device_id_type=MESH,
        )

    def came(way, half, distance):
        ag_copy(way, half, distance - 1, arriving=True).wait_recv()
        if distance < (4 if half == way else 3):
            ag_copy(way, half, distance).start()
        offset = 4 if distance == 4 else -distance * (1 - 2 * way)
        share_copy(offset, half).start()

    def feed(offset):
        for half in range(2):
            share_copy(offset, half, arriving=True).wait_recv()

    def experts(first, count):
        def step(number, carry):
            chip = ex.chip(first - 2 * first * number)
            piece = xbuf[pl.ds(chip * 2, 2)].reshape(4 * part, xbuf.shape[2])
            gated = dot32(piece, gate[0])
            upward = dot32(piece, up[0])
            hidden = (jax.nn.silu(gated) * upward).astype(jnp.bfloat16)
            for begin in range(0, xbuf.shape[2], 512):
                cols = slice(begin, begin + 512)
                term = dot32(hidden, down[0, :, cols]).astype(jnp.bfloat16)
                pbuf[pl.ds(chip * 2, 2), :, cols] = term.reshape(2, 2 * part, 512)
            return carry

        lax.fori_loop(0, count, step, 0)

    for way in range(2):
        ag_copy(way, way, 0).start()
        ag_copy(way, 1 - way, 0).start()
    for half in range(2):
        share_copy(0, half).start()
    for distance in (1, 2, 3):
        came(0, 0, distance)
        came(1, 1, distance)
        came(0, 1, distance)
        came(1, 0, distance)
        if distance == 1:
            for load in loads:
                load.wait()
            feed(0)
            experts(0, 1)
            ex.pair_copy(0).start()
        else:
            feed(1 - distance)
            feed(distance - 1)
            experts(distance - 1, 2)
            ex.pair_copy(1 - distance).start()
            ex.pair_copy(distance - 1).start()
    feed(-3)
    feed(3)
    experts(3, 2)
    ex.pair_copy(-3).start()
    ex.pair_copy(3).start()
    came(0, 0, 4)
    came(1, 1, 4)
    ex.pair_copy(3).wait_recv()
    ex.send(0, 1, 3)
    ex.pair_copy(-3).wait_recv()
    ex.send(1, 0, 3)
    feed(4)
    experts(4, 1)
    ex.pair_copy(4).start()
    for offset in (2, -2, 1, -1, 0, 4):
        ex.pair_copy(offset).wait_recv()
    ex.send(0, 0, 4)
    ex.send(1, 1, 4)
    for distance in (3, 2, 1):
        if distance < 3:
            ex.send(0, 1, distance)
            ex.send(1, 0, distance)
        ex.send(0, 0, distance)
        ex.send(1, 1, distance)
    for half in range(2):
        out_ref[half * part : (half + 1) * part, :] = ex.last(half).astype(jnp.bfloat16)
    ex.finish()
    for way in range(2):
        for half in range(2):
            for distance in range(4 if half == way else 3):
                ag_copy(way, half, distance).wait_send()
    for offset in range(-3, 5):
        for half in range(2):
            share_copy(offset, half).wait_send()


def run_experts(rows, gate, up, down):
    count, width = rows.shape
    vmem = pl.BlockSpec(memory_space=pltpu.VMEM)
    anywhere = pl.BlockSpec(memory_space=pl.ANY)
    return pl.pallas_call(
        expert_kernel,
        out_shape=jax.ShapeDtypeStruct((count, width), jnp.bfloat16),
        in_specs=[vmem, anywhere, anywhere, anywhere],
        out_specs=vmem,
        scratch_shapes=[
            pltpu.VMEM((16, count, width), jnp.bfloat16),
            pltpu.VMEM(gate.shape, gate.dtype),
            pltpu.VMEM(up.shape, up.dtype),
            pltpu.VMEM(down.shape, down.dtype),
            pltpu.SemaphoreType.DMA((3,)),
            pltpu.SemaphoreType.DMA((16,)),
            pltpu.SemaphoreType.DMA((16,)),
            pltpu.SemaphoreType.DMA((16,)),
            pltpu.SemaphoreType.DMA((16,)),
        ]
        + exchange_scratch(count, width),
        compiler_params=pltpu.CompilerParams(
            collective_id=2, has_side_effects=True, vmem_limit_bytes=60 * 1024 * 1024
        ),
    )(rows, gate, up, down)


def per_device(
    resid,
    query_a,
    key_a,
    value_a,
    query_b,
    key_b,
    value_b,
    mix_a,
    mix_b,
    head_gain_a,
    head_gain_b,
    proj_a,
    proj_b,
    norm_gain,
    route_ids,
    route_weights,
    expert_gate,
    expert_up,
    expert_down,
):
    sp_ways = lax.axis_size("sp")
    heads_out = attention(
        query_a, key_a, value_a, query_b, key_b, value_b, mix_a, mix_b, head_gain_a, head_gain_b
    )
    width = resid.shape[1]
    tok_rows = resid.shape[0]
    top_count = route_ids.shape[1]
    capacity = 3 * top_count * tok_rows // (2 * sp_ways)
    own_slots = slot_numbers(route_ids, sp_ways, capacity)
    lookup = jnp.arange(sp_ways * capacity, dtype=jnp.int32)[:, None]
    spread = jnp.zeros((sp_ways * capacity, tok_rows), jnp.float32)
    for which in range(top_count):
        spread = spread + (own_slots[:, which][None, :] == lookup).astype(jnp.float32)
    mixed, outgoing = project(
        heads_out, proj_a, proj_b, resid, norm_gain, spread.astype(jnp.bfloat16)
    )
    arrived = lax.all_to_all(
        outgoing.reshape(sp_ways, capacity, width), "sp", split_axis=0, concat_axis=0, tiled=True
    )
    summed = run_experts(
        arrived.reshape(sp_ways * capacity, width), expert_gate, expert_up, expert_down
    )
    finished_rows = summed.reshape(sp_ways, capacity, width)
    back = lax.all_to_all(finished_rows, "sp", split_axis=0, concat_axis=0, tiled=True)
    picked = jnp.take(back.reshape(sp_ways * capacity, width), own_slots.reshape(-1), axis=0)
    picked = picked.reshape(tok_rows, top_count, width)
    output = mixed + jnp.sum(route_weights[:, :, None] * picked.astype(jnp.float32), axis=1)
    return output.astype(jnp.bfloat16)


def solution(mesh):
    placed = (
        P(("sp", "tp"), None),
        P("sp", "tp", None),
        P("sp", "tp", None),
        P("sp", "tp", None),
        P("sp", "tp", None),
        P("sp", "tp", None),
        P("sp", "tp", None),
        P("tp"),
        P("tp"),
        P(),
        P(),
        P("tp", None),
        P("tp", None),
        P(),
        P(("sp", "tp"), None),
        P(("sp", "tp"), None),
        P("sp", None, "tp"),
        P("sp", None, "tp"),
        P("sp", "tp", None),
    )
    return jax.shard_map(
        per_device, mesh=mesh, in_specs=placed, out_specs=P(("sp", "tp"), None), check_vma=False
    )
```

```python
import math

import jax
import jax.numpy as jnp
from jax import lax
from jax.experimental import pallas as pl
from jax.experimental.pallas import tpu as pltpu
from jax.sharding import PartitionSpec as P

EPS = 1e-06
NEG = -1e30
HEAD_SCALE = 1.0 - (0.8 - 0.6 * math.exp(-0.3))


def rms_scaled(values, gain):
    return values * lax.rsqrt(jnp.mean(values * values, axis=-1, keepdims=True) + EPS) * gain


MESH = pl.DeviceIdType.MESH
LOG2E = 1.4426950408889634
PART = 128
CHUNK = 64


def dot32(a, b):
    return jnp.dot(a, b, preferred_element_type=jnp.float32)


def attention_kernel(
    qa_ref, qb_ref, ka_ref, va_ref, kb_ref, vb_ref, mix_a_ref, mix_b_ref, gain_a_ref, gain_b_ref,
    out_ref,
    buf, qta, qtb, k_b, s_even, s_odd, p_even, p_odd, acc_a, acc_b, m_ref, l_ref,
    send_sem, recv_sem,
):
    s_refs, p_refs = (s_even, s_odd), (p_even, p_odd)
    place = lax.axis_index("sp")
    tp = lax.axis_index("tp")
    y, x = place // 4, place % 4
    half = buf.shape[2]

    def at(ox, oy):
        return ((y + oy + 4) % 4) * 4 + (x + ox + 4) % 4

    def spot(h, df, dg):
        return at(df, dg) if h == 0 else at(dg, df)

    barrier = pltpu.get_barrier_semaphore()
    for ox, oy in ((1, 0), (-1, 0), (0, 1), (0, -1)):
        pl.semaphore_signal(barrier, inc=1, device_id=(at(ox, oy), tp), device_id_type=MESH)

    va_t = jnp.transpose(va_ref[...])
    for h in range(2):
        cols = slice(h * half, (h + 1) * half)
        buf[place, h, :, 0:128] = ka_ref[cols, :]
        buf[place, h, 0:128, 128:384] = va_t[:, cols]
        buf[place, h, 128:192, 128:384] = kb_ref[:, cols]
        buf[place, h, 192:256, 128:384] = vb_ref[:, cols]

    pl.semaphore_wait(barrier, 4)

    def region(h, df, dg, part):
        ref = buf.at[spot(h, df, dg), h]
        return ref if part is None else ref.at[pl.ds(part * PART, PART)]

    def copy(h, number, df, dg, part, to_f, to_g):
        ref = region(h, df, dg, part)
        return pltpu.make_async_remote_copy(
            src_ref=ref,
            dst_ref=ref,
            send_sem=send_sem.at[h * 20 + number],
            recv_sem=recv_sem.at[h * 20 + number],
            device_id=(spot(h, to_f, to_g), tp),
            device_id_type=MESH,
        )

    moves = {
        0: (0, 0, None, 1, 0), 1: (0, 0, None, -1, 0),
        2: (0, 0, None, 0, 1), 3: (0, 0, None, 0, -1),
        4: (-1, 0, 0, 1, 0), 5: (1, 0, 1, -1, 0),
        6: (-1, 0, None, 0, 1), 7: (-1, 0, None, 0, -1),
        8: (1, 0, None, 0, 1), 9: (1, 0, None, 0, -1),
        10: (2, 0, None, 0, 1), 11: (2, 0, None, 0, -1),
        12: (0, -1, 0, 0, 1), 13: (0, 1, 1, 0, -1),
        14: (-1, -1, 0, 0, 1), 15: (-1, 1, 1, 0, -1),
        16: (1, -1, 0, 0, 1), 17: (1, 1, 1, 0, -1),
        18: (2, -1, 0, 0, 1), 19: (2, 1, 1, 0, -1),
    }

    def start(*numbers):
        for number in numbers:
            for h in range(2):
                copy(h, number, *moves[number]).start()

    def arrive(number, *then):
        df, dg, part, to_f, to_g = moves[number]
        for h in range(2):
            copy(h, number, df - to_f, dg - to_g, part, to_f, to_g).wait_recv()
            for follow in then:
                copy(h, follow, *moves[follow]).start()

    start(0, 1, 2, 3)

    qa_t = jnp.transpose(qa_ref[...])
    zero_a = jnp.zeros((64, half), jnp.bfloat16)
    zero_b = jnp.zeros((32, half), jnp.bfloat16)
    for h in range(2):
        cols = slice(h * half, (h + 1) * half)
        qta[h, 0:64, :] = qa_t[0:64, cols]
        qta[h, 64:128, :] = zero_a
        qta[2 + h, 0:64, :] = zero_a
        qta[2 + h, 64:128, :] = qa_t[64:128, cols]
        qtb[h, 0:32, :] = qb_ref[0:32, cols]
        qtb[h, 32:64, :] = zero_b
        qtb[2 + h, 0:32, :] = zero_b
        qtb[2 + h, 32:64, :] = qb_ref[32:64, cols]
    acc_a[...] = jnp.zeros_like(acc_a)
    acc_b[...] = jnp.zeros_like(acc_b)
    m_ref[...] = jnp.full_like(m_ref, NEG)
    l_ref[...] = jnp.zeros_like(l_ref)

    def score(number, source, offsets):
        index, group, place_in = number // 2, number % 2, number % 2
        top = None
        for h in range(2):
            keys = k_b[h] if group else buf[source, h, :, 0:128]
            found = dot32(keys, qtb[index] if group else qta[index])
            if offsets is not None:
                query_pos = (index % 2) * half + lax.broadcasted_iota(jnp.int32, (half, half), 1)
                key_pos = offsets[h] + lax.broadcasted_iota(jnp.int32, (half, half), 0)
                found = jnp.where(key_pos <= query_pos, found, NEG)
            s_refs[place_in][h * half : (h + 1) * half, :] = found
            most = jnp.max(found.reshape(half // 8, 8, half), axis=0)
            top = most if top is None else jnp.maximum(top, most)
        return jnp.max(top, axis=0, keepdims=True)

    def soften(number, top):
        index, group = number // 2, number % 2
        slot, factor = index + 4 * group, (LOG2E / math.sqrt(32.0) if group else LOG2E / 8.0)
        old = m_ref[slot]
        fresh = jnp.maximum(old, top)
        scale = jnp.exp2((old - fresh) * factor)
        m_ref[slot] = fresh
        sums = l_ref[slot] * scale
        for first in range(0, 2 * half, CHUNK):
            rows = slice(first, first + CHUNK)
            weights = jnp.exp2((s_refs[group][rows, :] - fresh) * factor)
            sums = sums + jnp.sum(weights.reshape(CHUNK // 8, 8, half), axis=0)
            p_refs[group][rows, :] = weights.astype(jnp.bfloat16)
        l_ref[slot] = sums
        return scale

    def gather(number, source, scale):
        index, group = number // 2, number % 2
        acc, rows = (acc_b, slice(192, 256)) if group else (acc_a, slice(0, 128))
        added = dot32(buf[source, 0, rows, 128:384], p_refs[group][0:half, :])
        added = added + dot32(buf[source, 1, rows, 128:384], p_refs[group][half : 2 * half, :])
        acc[index] = acc[index] * scale + added

    def block(source, offsets):
        for h in range(2):
            k_b[h] = jnp.transpose(buf[source, h, 128:192, 128:384])
        top = score(0, source, offsets)
        for number in range(8):
            later = score(number + 1, source, offsets) if number < 7 else None
            gather(number, source, soften(number, top))
            top = later

    plan = (
        ((-1, 0), ()), ((0, -1), (4, 5)), ((1, 0), ()), ((0, 1), (6, 7)), ((-1, -1), ()),
        ((1, -1), (8, 9)), ((-1, 1), ()), ((1, 1), ()), ((2, 0), (10, 11, 12, 13)), ((0, 2), ()),
        ((2, -1), (14, 15)), ((-1, 2), ()), ((2, 1), (16, 17)), ((1, 2), ()), ((2, 2), (18, 19)),
    )
    follow = {5: (10, 11), 6: (14,), 7: (15,), 8: (16,), 9: (17,), 10: (18,), 11: (19,)}

    def step(number, carry):
        ox, oy = jnp.int32(0), jnp.int32(0)
        for which, ((dx, dy), events) in enumerate(plan):
            ox = jnp.where(number == which, dx, ox)
            oy = jnp.where(number == which, dy, oy)
            if events:

                @pl.when(number == which)
                def _(events=events):
                    for event in events:
                        arrive(event, *follow.get(event, ()))

        source = at(ox, oy)

        @pl.when(source < place)
        def _():
            block(source, None)

        return carry

    block(place, (0, half))
    arrive(0, 4, 6, 7)
    arrive(1, 5, 8, 9)
    arrive(2, 12)
    arrive(3, 13)
    lax.fori_loop(0, len(plan), step, 0)

    for h in range(2):
        for acc, base, mix, gain, first in (
            (acc_a, 0, mix_a_ref, gain_a_ref, 0), (acc_b, 4, mix_b_ref, gain_b_ref, 128),
        ):
            one = acc[h] / jnp.sum(l_ref[base + h], axis=0, keepdims=True)
            two = acc[2 + h] / jnp.sum(l_ref[base + 2 + h], axis=0, keepdims=True)
            mixed = one - mix[0] * two
            mixed = mixed * lax.rsqrt(jnp.mean(mixed * mixed, axis=0, keepdims=True) + EPS)
            rows = jnp.transpose(mixed) * gain[...] * HEAD_SCALE
            out_ref[h * half : (h + 1) * half, first : first + rows.shape[1]] = rows.astype(
                jnp.bfloat16
            )
    for number in range(20):
        for h in range(2):
            copy(h, number, *moves[number]).wait_send()


def attention(query_a, key_a, value_a, query_b, key_b, value_b, mix_a, mix_b, gain_a, gain_b):
    rows = query_a.shape[0]
    vmem = pl.BlockSpec(memory_space=pltpu.VMEM)
    return pl.pallas_call(
        attention_kernel,
        out_shape=jax.ShapeDtypeStruct((rows, 192), jnp.bfloat16),
        in_specs=[vmem] * 6 + [pl.BlockSpec(memory_space=pltpu.SMEM)] * 2 + [vmem] * 2,
        out_specs=vmem,
        scratch_shapes=[
            pltpu.VMEM((16, 2, 256, 384), jnp.bfloat16),
            pltpu.VMEM((4, 128, 256), jnp.bfloat16),
            pltpu.VMEM((4, 64, 256), jnp.bfloat16),
            pltpu.VMEM((2, 256, 64), jnp.bfloat16),
            pltpu.VMEM((512, 256), jnp.float32),
            pltpu.VMEM((512, 256), jnp.float32),
            pltpu.VMEM((512, 256), jnp.bfloat16),
            pltpu.VMEM((512, 256), jnp.bfloat16),
            pltpu.VMEM((4, 128, 256), jnp.float32),
            pltpu.VMEM((4, 64, 256), jnp.float32),
            pltpu.VMEM((8, 1, 256), jnp.float32),
            pltpu.VMEM((8, 8, 256), jnp.float32),
            pltpu.SemaphoreType.DMA((40,)),
            pltpu.SemaphoreType.DMA((40,)),
        ],
        compiler_params=pltpu.CompilerParams(collective_id=0, has_side_effects=True),
    )(
        query_a[:, 0, :], query_b[:, 0, :].T, key_a[:, 0, :], value_a[:, 0, :],
        key_b[:, 0, :].T, value_b[:, 0, :].T,
        mix_a, mix_b, gain_a[None, :], gain_b[None, :],
    )


def tp_place():
    tp = lax.axis_index("tp")
    return lax.axis_index("sp"), tp // 2, tp % 2


def meet(sp, z, core):
    tp = z * 2 + core
    barrier = pltpu.get_barrier_semaphore()
    peers = [(sp, ((z + 1) % 8) * 2 + core), (sp, ((z + 7) % 8) * 2 + core), (sp, tp + 1 - 2 * core)]
    peers += [((sp + delta) % 16, tp) for delta in range(1, 16)]
    for peer in peers:
        pl.semaphore_signal(barrier, inc=1, device_id=peer, device_id_type=MESH)
    pl.semaphore_wait(barrier, len(peers))


class Exchange:
    def __init__(self, pbuf, other, stage, landed, pair_send, pair_recv, ring_send, ring_recv):
        self.sp, self.z, self.core = tp_place()
        self.pbuf, self.other, self.stage, self.landed = pbuf, other, stage, landed
        self.pair_sems, self.ring_sems = (pair_send, pair_recv), (ring_send, ring_recv)
        self.rows = pbuf.shape[1] // 2

    def chip(self, offset):
        return (self.z + offset + 8) % 8

    def pair_copy(self, offset):
        chip = self.chip(offset)
        return pltpu.make_async_remote_copy(
            src_ref=self.pbuf.at[chip * 2 + 1 - self.core],
            dst_ref=self.other.at[chip],
            send_sem=self.pair_sems[0].at[offset + 3],
            recv_sem=self.pair_sems[1].at[offset + 3],
            device_id=(self.sp, self.z * 2 + 1 - self.core),
            device_id_type=MESH,
        )

    def ring_copy(self, way, half, distance):
        number = way * 8 + half * 4 + distance - 1
        return pltpu.make_async_remote_copy(
            src_ref=self.stage.at[way, half, distance - 1],
            dst_ref=self.landed.at[way, half, distance - 1],
            send_sem=self.ring_sems[0].at[number],
            recv_sem=self.ring_sems[1].at[number],
            device_id=(self.sp, self.chip(1 - 2 * way) * 2 + self.core),
            device_id_type=MESH,
        )

    def mine(self, offset, half):
        chip = self.chip(offset)
        rows = slice(half * self.rows, (half + 1) * self.rows)
        own = self.pbuf[chip * 2 + self.core, rows, :].astype(jnp.float32)
        return own + self.other[chip, rows, :].astype(jnp.float32)

    def send(self, way, half, distance):
        offset = distance * (1 - 2 * way)
        total = self.mine(4 if distance == 4 else offset, half)
        if distance < (4 if half == way else 3):
            self.ring_copy(way, half, distance + 1).wait_recv()
            total = total + self.landed[way, half, distance].astype(jnp.float32)
        self.stage[way, half, distance - 1] = total.astype(jnp.bfloat16)
        self.ring_copy(way, half, distance).start()

    def last(self, half):
        total = self.mine(0, half)
        for way in range(2):
            self.ring_copy(way, half, 1).wait_recv()
            total = total + self.landed[way, half, 0].astype(jnp.float32)
        return total

    def finish(self):
        for offset in range(-3, 5):
            self.pair_copy(offset).wait_send()
        for way in range(2):
            for half in range(2):
                for distance in range(1, 5 if half == way else 4):
                    self.ring_copy(way, half, distance).wait_send()


def exchange_scratch(rows, width):
    return [
        pltpu.VMEM((16, rows, width), jnp.bfloat16),
        pltpu.VMEM((8, rows, width), jnp.bfloat16),
        pltpu.VMEM((2, 2, 4, rows // 2, width), jnp.bfloat16),
        pltpu.VMEM((2, 2, 4, rows // 2, width), jnp.bfloat16),
        pltpu.SemaphoreType.DMA((8,)),
        pltpu.SemaphoreType.DMA((8,)),
        pltpu.SemaphoreType.DMA((16,)),
        pltpu.SemaphoreType.DMA((16,)),
    ]


SLAB = 8


def slab_copy(slabs, landing, delta, send_sem, recv_sem, arriving=False):
    sp, tp = lax.axis_index("sp"), lax.axis_index("tp")
    there = (sp + delta) % 16
    return pltpu.make_async_remote_copy(
        src_ref=slabs.at[there],
        dst_ref=landing.at[(sp + 16 - delta) % 16 if arriving else sp],
        send_sem=send_sem.at[delta],
        recv_sem=recv_sem.at[delta],
        device_id=(there, tp),
        device_id_type=MESH,
    )


def chosen_slots(ids_ref):
    tokens = ids_ref.shape[1]
    expert = lax.broadcasted_iota(jnp.int32, (16, tokens), 0)
    named = [(expert == ids_ref[r : r + 1, :]).astype(jnp.float32) for r in range(2)]
    earlier = lax.broadcasted_iota(jnp.int32, (tokens, tokens), 0)
    earlier = (earlier < lax.broadcasted_iota(jnp.int32, (tokens, tokens), 1)).astype(jnp.bfloat16)
    before = dot32((named[0] + named[1]).astype(jnp.bfloat16), earlier)
    slots = lax.broadcasted_iota(jnp.int32, (16 * SLAB, tokens), 0)
    result = []
    for r in range(2):
        rank = jnp.sum(named[r] * before, axis=0, keepdims=True).astype(jnp.int32)
        result.append((slots == ids_ref[r : r + 1, :] * SLAB + rank).astype(jnp.bfloat16))
    return result


def packing(rows, capacity):
    shape = (rows, rows // capacity * SLAB)
    row = lax.broadcasted_iota(jnp.int32, shape, 0)
    column = lax.broadcasted_iota(jnp.int32, shape, 1)
    used = column % SLAB < capacity
    return (used & (row == column // SLAB * capacity + column % SLAB)).astype(jnp.bfloat16)


def unpacking(rows, capacity):
    shape = (rows // capacity * SLAB, rows)
    row = lax.broadcasted_iota(jnp.int32, shape, 0)
    column = lax.broadcasted_iota(jnp.int32, shape, 1)
    used = row % SLAB < capacity
    return (used & (column == row // SLAB * capacity + row % SLAB)).astype(jnp.bfloat16)


def experts_kernel(
    heads_ref, proj_a_ref, proj_b_ref, resid_ref, gain_ref, ids_ref, weights_ref,
    gate_hbm, up_hbm, down_hbm, out_ref,
    mixed, slabs, landing, returned, back, go_send, go_recv, back_send, back_recv,
    xbuf, gate, up, down, w_sem, ag_send, ag_recv, share_send, share_recv, *exchange,
):
    sp, z, core = tp_place()
    px = Exchange(*exchange[:8])
    ex = Exchange(*exchange[8:])
    width = mixed.shape[1]
    loads = [
        pltpu.make_async_copy(src, dst, w_sem.at[i])
        for i, (src, dst) in enumerate(((gate_hbm, gate), (up_hbm, up), (down_hbm, down)))
    ]
    for load in loads:
        load.start()
    pbuf = ex.pbuf
    for first in range(0, width, 512):
        cols = slice(first, first + 512)
        term = dot32(heads_ref[:, 0:128], proj_a_ref[:, cols])
        term = term + dot32(heads_ref[:, 128:192], proj_b_ref[:, cols])
        px.pbuf[:, :, cols] = term.astype(jnp.bfloat16).reshape(16, 32, 512)
    meet(sp, z, core)
    for offset in (4, 3, -3, 2, -2, 1, -1, 0):
        px.pair_copy(offset).start()
    chosen = chosen_slots(ids_ref)
    px.pair_copy(4).wait_recv()
    px.send(0, 0, 4)
    px.send(1, 1, 4)
    for distance in (3, 2, 1):
        px.pair_copy(distance).wait_recv()
        px.pair_copy(-distance).wait_recv()
        if distance == 3:
            px.send(0, 1, 3)
            px.send(1, 0, 3)
        px.send(0, 0, distance)
        px.send(1, 1, distance)
        if distance < 3:
            px.send(0, 1, distance)
            px.send(1, 0, distance)
    px.pair_copy(0).wait_recv()
    for half in range(2):
        rows = slice(half * 16, half * 16 + 16)
        mixed[rows, :] = resid_ref[rows, :].astype(jnp.float32) + px.last(half)
    normed = rms_scaled(mixed[...], gain_ref[...]).astype(jnp.bfloat16)
    outgoing = dot32(chosen[0] + chosen[1], normed).astype(jnp.bfloat16)
    slabs[...] = outgoing.reshape(16, SLAB, width)
    for delta in range(1, 16):
        slab_copy(slabs, landing, delta, go_send, go_recv).start()
    landing[sp] = slabs[sp]
    for delta in range(1, 16):
        slab_copy(slabs, landing, delta, go_send, go_recv, arriving=True).wait_recv()
    count = xbuf.shape[1]
    capacity = count // 16
    arrived = landing[...].reshape(16 * SLAB, width)
    xbuf[z * 2 + core] = dot32(packing(count, capacity), arrived).astype(jnp.bfloat16)
    part = count // 2

    def shard(offset, half):
        chip = ex.chip(offset)
        return xbuf.at[chip * 2 + core, pl.ds(half * part, part)]

    def ag_copy(way, half, distance, arriving=False):
        sign = 1 - 2 * way
        away = distance + 1 if arriving else distance
        offset = 4 if away == 4 else -sign * away
        number = way * 8 + half * 4 + distance
        return pltpu.make_async_remote_copy(
            src_ref=shard(offset, half),
            dst_ref=shard(offset, half),
            send_sem=ag_send.at[number],
            recv_sem=ag_recv.at[number],
            device_id=(sp, ex.chip(sign) * 2 + core),
            device_id_type=MESH,
        )

    def share_copy(offset, half, arriving=False):
        chip = ex.chip(offset)
        there = xbuf.at[chip * 2 + (1 - core if arriving else core), pl.ds(half * part, part)]
        number = (offset + 3) * 2 + half
        return pltpu.make_async_remote_copy(
            src_ref=there,
            dst_ref=there,
            send_sem=share_send.at[number],
            recv_sem=share_recv.at[number],
            device_id=(sp, z * 2 + 1 - core),
            device_id_type=MESH,
        )

    def came(way, half, distance):
        ag_copy(way, half, distance - 1, arriving=True).wait_recv()
        if distance < (4 if half == way else 3):
            ag_copy(way, half, distance).start()
        offset = 4 if distance == 4 else -distance * (1 - 2 * way)
        share_copy(offset, half).start()

    def feed(offset):
        for half in range(2):
            share_copy(offset, half, arriving=True).wait_recv()

    def experts(first, count):
        def step(number, carry):
            chip = ex.chip(first - 2 * first * number)
            piece = xbuf[pl.ds(chip * 2, 2)].reshape(4 * part, xbuf.shape[2])
            gated = dot32(piece, gate[0])
            upward = dot32(piece, up[0])
            hidden = (jax.nn.silu(gated) * upward).astype(jnp.bfloat16)
            for begin in range(0, xbuf.shape[2], 512):
                cols = slice(begin, begin + 512)
                term = dot32(hidden, down[0, :, cols]).astype(jnp.bfloat16)
                pbuf[pl.ds(chip * 2, 2), :, cols] = term.reshape(2, 2 * part, 512)
            return carry

        lax.fori_loop(0, count, step, 0)

    for way in range(2):
        ag_copy(way, way, 0).start()
        ag_copy(way, 1 - way, 0).start()
    for half in range(2):
        share_copy(0, half).start()
    for distance in (1, 2, 3):
        came(0, 0, distance)
        came(1, 1, distance)
        came(0, 1, distance)
        came(1, 0, distance)
        if distance == 1:
            for load in loads:
                load.wait()
            feed(0)
            experts(0, 1)
            ex.pair_copy(0).start()
        else:
            feed(1 - distance)
            feed(distance - 1)
            experts(distance - 1, 2)
            ex.pair_copy(1 - distance).start()
            ex.pair_copy(distance - 1).start()
    feed(-3)
    feed(3)
    experts(3, 2)
    ex.pair_copy(-3).start()
    ex.pair_copy(3).start()
    came(0, 0, 4)
    came(1, 1, 4)
    ex.pair_copy(3).wait_recv()
    ex.send(0, 1, 3)
    ex.pair_copy(-3).wait_recv()
    ex.send(1, 0, 3)
    feed(4)
    experts(4, 1)
    ex.pair_copy(4).start()
    for offset in (2, -2, 1, -1, 0, 4):
        ex.pair_copy(offset).wait_recv()
    ex.send(0, 0, 4)
    ex.send(1, 1, 4)
    for distance in (3, 2, 1):
        if distance < 3:
            ex.send(0, 1, distance)
            ex.send(1, 0, distance)
        ex.send(0, 0, distance)
        ex.send(1, 1, distance)
    widen = unpacking(part, capacity)
    for half in range(2):
        summed = ex.last(half).astype(jnp.bfloat16)
        spread = dot32(widen, summed).astype(jnp.bfloat16)
        returned[half * 8 : half * 8 + 8] = spread.reshape(8, SLAB, width)
    for delta in range(1, 16):
        slab_copy(returned, back, delta, back_send, back_recv).start()
    back[sp] = returned[sp]
    tokens = mixed.shape[0]
    row = lax.broadcasted_iota(jnp.int32, (tokens, tokens), 0)
    same = row == lax.broadcasted_iota(jnp.int32, (tokens, tokens), 1)
    picks = [jnp.transpose(c.astype(jnp.float32)).astype(jnp.bfloat16) for c in chosen]
    factors = [
        jnp.sum(jnp.where(same, weights_ref[r : r + 1, :], 0.0), axis=1, keepdims=True)
        for r in range(2)
    ]
    for delta in range(1, 16):
        slab_copy(returned, back, delta, back_send, back_recv, arriving=True).wait_recv()
    rows = back[...].reshape(16 * SLAB, width)
    added = factors[0] * dot32(picks[0], rows) + factors[1] * dot32(picks[1], rows)
    out_ref[...] = (mixed[...] + added).astype(jnp.bfloat16)
    for delta in range(1, 16):
        slab_copy(slabs, landing, delta, go_send, go_recv).wait_send()
        slab_copy(returned, back, delta, back_send, back_recv).wait_send()
    px.finish()
    ex.finish()
    for way in range(2):
        for half in range(2):
            for distance in range(4 if half == way else 3):
                ag_copy(way, half, distance).wait_send()
    for offset in range(-3, 5):
        for half in range(2):
            share_copy(offset, half).wait_send()


def project_and_run_experts(
    heads_out, proj_a, proj_b, resid, norm_gain, route_ids, route_weights, gate, up, down
):
    tokens, width = resid.shape
    count = 3 * route_ids.shape[1] * tokens // 2
    vmem = pl.BlockSpec(memory_space=pltpu.VMEM)
    anywhere = pl.BlockSpec(memory_space=pl.ANY)
    return pl.pallas_call(
        experts_kernel,
        out_shape=jax.ShapeDtypeStruct((tokens, width), jnp.bfloat16),
        in_specs=[vmem] * 7 + [anywhere] * 3,
        out_specs=vmem,
        scratch_shapes=[pltpu.VMEM((tokens, width), jnp.float32)]
        + [pltpu.VMEM((16, SLAB, width), jnp.bfloat16)] * 4
        + [pltpu.SemaphoreType.DMA((16,))] * 4
        + [
            pltpu.VMEM((16, count, width), jnp.bfloat16),
            pltpu.VMEM(gate.shape, gate.dtype),
            pltpu.VMEM(up.shape, up.dtype),
            pltpu.VMEM(down.shape, down.dtype),
            pltpu.SemaphoreType.DMA((3,)),
        ]
        + [pltpu.SemaphoreType.DMA((16,))] * 4
        + exchange_scratch(tokens, width)
        + exchange_scratch(count, width),
        compiler_params=pltpu.CompilerParams(
            collective_id=1, has_side_effects=True, vmem_limit_bytes=60 * 1024 * 1024
        ),
    )(
        heads_out, proj_a, proj_b, resid, norm_gain[None, :], route_ids.T, route_weights.T,
        gate, up, down,
    )


def per_device(
    resid,
    query_a,
    key_a,
    value_a,
    query_b,
    key_b,
    value_b,
    mix_a,
    mix_b,
    head_gain_a,
    head_gain_b,
    proj_a,
    proj_b,
    norm_gain,
    route_ids,
    route_weights,
    expert_gate,
    expert_up,
    expert_down,
):
    heads_out = attention(
        query_a, key_a, value_a, query_b, key_b, value_b, mix_a, mix_b, head_gain_a, head_gain_b
    )
    return project_and_run_experts(
        heads_out, proj_a, proj_b, resid, norm_gain, route_ids, route_weights,
        expert_gate, expert_up, expert_down,
    )


def solution(mesh):
    placed = (
        P(("sp", "tp"), None),
        P("sp", "tp", None),
        P("sp", "tp", None),
        P("sp", "tp", None),
        P("sp", "tp", None),
        P("sp", "tp", None),
        P("sp", "tp", None),
        P("tp"),
        P("tp"),
        P(),
        P(),
        P("tp", None),
        P("tp", None),
        P(),
        P(("sp", "tp"), None),
        P(("sp", "tp"), None),
        P("sp", None, "tp"),
        P("sp", None, "tp"),
        P("sp", "tp", None),
    )
    return jax.shard_map(
        per_device, mesh=mesh, in_specs=placed, out_specs=P(("sp", "tp"), None), check_vma=False
    )
```

```python
import math

import jax
import jax.numpy as jnp
from jax import lax
from jax.experimental import pallas as pl
from jax.experimental.pallas import tpu as pltpu
from jax.sharding import PartitionSpec as P

EPS = 1e-06
NEG = -1e30
HEAD_SCALE = 1.0 - (0.8 - 0.6 * math.exp(-0.3))


def rms_scaled(values, gain):
    return values * lax.rsqrt(jnp.mean(values * values, axis=-1, keepdims=True) + EPS) * gain


MESH = pl.DeviceIdType.MESH
LOG2E = 1.4426950408889634
PART = 128
CHUNK = 64
PIECES = 2


def dot32(a, b):
    return jnp.dot(a, b, preferred_element_type=jnp.float32)


def attention_part(
    qa_ref, qb_ref, ka_ref, va_ref, kb_ref, vb_ref, mix_a_ref, mix_b_ref, gain_a_ref, gain_b_ref,
    out_ref,
    buf, qta, qtb, k_b, s_even, s_odd, p_even, p_odd, acc_a, acc_b, m_ref, l_ref,
    send_sem, recv_sem,
):
    s_refs, p_refs = (s_even, s_odd), (p_even, p_odd)
    place = lax.axis_index("sp")
    tp = lax.axis_index("tp")
    y, x = place // 4, place % 4
    half = buf.shape[2]

    def at(ox, oy):
        return ((y + oy + 4) % 4) * 4 + (x + ox + 4) % 4

    def spot(h, df, dg):
        return at(df, dg) if h == 0 else at(dg, df)

    peers = greet()

    va_t = jnp.transpose(va_ref[...])
    for h in range(2):
        cols = slice(h * half, (h + 1) * half)
        buf[place, h, :, 0:128] = ka_ref[cols, :]
        buf[place, h, 0:128, 128:384] = va_t[:, cols]
        buf[place, h, 128:192, 128:384] = kb_ref[:, cols]
        buf[place, h, 192:256, 128:384] = vb_ref[:, cols]

    pl.semaphore_wait(pltpu.get_barrier_semaphore(), peers)

    def region(h, df, dg, part):
        ref = buf.at[spot(h, df, dg), h]
        return ref if part is None else ref.at[pl.ds(part * PART, PART)]

    def copy(h, number, df, dg, part, to_f, to_g):
        ref = region(h, df, dg, part)
        return pltpu.make_async_remote_copy(
            src_ref=ref,
            dst_ref=ref,
            send_sem=send_sem.at[h * 20 + number],
            recv_sem=recv_sem.at[h * 20 + number],
            device_id=(spot(h, to_f, to_g), tp),
            device_id_type=MESH,
        )

    moves = {
        0: (0, 0, None, 1, 0), 1: (0, 0, None, -1, 0),
        2: (0, 0, None, 0, 1), 3: (0, 0, None, 0, -1),
        4: (-1, 0, 0, 1, 0), 5: (1, 0, 1, -1, 0),
        6: (-1, 0, None, 0, 1), 7: (-1, 0, None, 0, -1),
        8: (1, 0, None, 0, 1), 9: (1, 0, None, 0, -1),
        10: (2, 0, None, 0, 1), 11: (2, 0, None, 0, -1),
        12: (0, -1, 0, 0, 1), 13: (0, 1, 1, 0, -1),
        14: (-1, -1, 0, 0, 1), 15: (-1, 1, 1, 0, -1),
        16: (1, -1, 0, 0, 1), 17: (1, 1, 1, 0, -1),
        18: (2, -1, 0, 0, 1), 19: (2, 1, 1, 0, -1),
    }

    def start(*numbers):
        for number in numbers:
            for h in range(2):
                copy(h, number, *moves[number]).start()

    def arrive(number, *then):
        df, dg, part, to_f, to_g = moves[number]
        for h in range(2):
            copy(h, number, df - to_f, dg - to_g, part, to_f, to_g).wait_recv()
            for follow in then:
                copy(h, follow, *moves[follow]).start()

    start(0, 1, 2, 3)

    qa_t = jnp.transpose(qa_ref[...])
    zero_a = jnp.zeros((64, half), jnp.bfloat16)
    zero_b = jnp.zeros((32, half), jnp.bfloat16)
    for h in range(2):
        cols = slice(h * half, (h + 1) * half)
        qta[h, 0:64, :] = qa_t[0:64, cols]
        qta[h, 64:128, :] = zero_a
        qta[2 + h, 0:64, :] = zero_a
        qta[2 + h, 64:128, :] = qa_t[64:128, cols]
        qtb[h, 0:32, :] = qb_ref[0:32, cols]
        qtb[h, 32:64, :] = zero_b
        qtb[2 + h, 0:32, :] = zero_b
        qtb[2 + h, 32:64, :] = qb_ref[32:64, cols]
    acc_a[...] = jnp.zeros_like(acc_a)
    acc_b[...] = jnp.zeros_like(acc_b)
    m_ref[...] = jnp.full_like(m_ref, NEG)
    l_ref[...] = jnp.zeros_like(l_ref)

    def score(number, source, offsets):
        index, group, place_in = number // 2, number % 2, number % 2
        top = None
        for h in range(2):
            keys = k_b[h] if group else buf[source, h, :, 0:128]
            found = dot32(keys, qtb[index] if group else qta[index])
            if offsets is not None:
                query_pos = (index % 2) * half + lax.broadcasted_iota(jnp.int32, (half, half), 1)
                key_pos = offsets[h] + lax.broadcasted_iota(jnp.int32, (half, half), 0)
                found = jnp.where(key_pos <= query_pos, found, NEG)
            s_refs[place_in][h * half : (h + 1) * half, :] = found
            most = jnp.max(found.reshape(half // 8, 8, half), axis=0)
            top = most if top is None else jnp.maximum(top, most)
        return jnp.max(top, axis=0, keepdims=True)

    def soften(number, top):
        index, group = number // 2, number % 2
        slot, factor = index + 4 * group, (LOG2E / math.sqrt(32.0) if group else LOG2E / 8.0)
        old = m_ref[slot]
        fresh = jnp.maximum(old, top)
        scale = jnp.exp2((old - fresh) * factor)
        m_ref[slot] = fresh
        sums = l_ref[slot] * scale
        for first in range(0, 2 * half, CHUNK):
            rows = slice(first, first + CHUNK)
            weights = jnp.exp2((s_refs[group][rows, :] - fresh) * factor)
            sums = sums + jnp.sum(weights.reshape(CHUNK // 8, 8, half), axis=0)
            p_refs[group][rows, :] = weights.astype(jnp.bfloat16)
        l_ref[slot] = sums
        return scale

    def gather(number, source, scale):
        index, group = number // 2, number % 2
        acc, rows = (acc_b, slice(192, 256)) if group else (acc_a, slice(0, 128))
        added = dot32(buf[source, 0, rows, 128:384], p_refs[group][0:half, :])
        added = added + dot32(buf[source, 1, rows, 128:384], p_refs[group][half : 2 * half, :])
        acc[index] = acc[index] * scale + added

    def block(source, offsets):
        for h in range(2):
            k_b[h] = jnp.transpose(buf[source, h, 128:192, 128:384])
        top = score(0, source, offsets)
        for number in range(8):
            later = score(number + 1, source, offsets) if number < 7 else None
            gather(number, source, soften(number, top))
            top = later

    plan = (
        ((-1, 0), ()), ((0, -1), (4, 5)), ((1, 0), ()), ((0, 1), (6, 7)), ((-1, -1), ()),
        ((2, 0), (12, 13)), ((0, 2), (8, 9)), ((1, -1), ()), ((-1, 1), ()), ((1, 1), ()),
        ((2, -1), (10, 11, 14, 15)), ((-1, 2), (16, 17)), ((2, 1), ()), ((1, 2), (18, 19)),
        ((2, 2), ()),
    )
    follow = {5: (10, 11), 6: (14,), 7: (15,), 8: (16,), 9: (17,), 10: (18,), 11: (19,)}

    def step(number, carry):
        ox, oy = jnp.int32(0), jnp.int32(0)
        for which, ((dx, dy), events) in enumerate(plan):
            ox = jnp.where(number == which, dx, ox)
            oy = jnp.where(number == which, dy, oy)
            if events:

                @pl.when(number == which)
                def _(events=events):
                    for event in events:
                        arrive(event, *follow.get(event, ()))

        source = at(ox, oy)

        @pl.when(source < place)
        def _():
            block(source, None)

        return carry

    block(place, (0, half))
    arrive(0, 4, 6, 7)
    arrive(1, 5)
    arrive(2, 12)
    arrive(3, 13, 8, 9)
    lax.fori_loop(0, len(plan), step, 0)

    for h in range(2):
        for acc, base, mix, gain, first in (
            (acc_a, 0, mix_a_ref, gain_a_ref, 0), (acc_b, 4, mix_b_ref, gain_b_ref, 128),
        ):
            one = acc[h] / jnp.sum(l_ref[base + h], axis=0, keepdims=True)
            two = acc[2 + h] / jnp.sum(l_ref[base + 2 + h], axis=0, keepdims=True)
            mixed = one - mix[0] * two
            mixed = mixed * lax.rsqrt(jnp.mean(mixed * mixed, axis=0, keepdims=True) + EPS)
            rows = jnp.transpose(mixed) * gain[...] * HEAD_SCALE
            out_ref[h * half : (h + 1) * half, first : first + rows.shape[1]] = rows.astype(
                jnp.bfloat16
            )

    def finish():
        for number in range(20):
            for h in range(2):
                copy(h, number, *moves[number]).wait_send()

    return finish


def tp_place():
    tp = lax.axis_index("tp")
    return lax.axis_index("sp"), tp // 2, tp % 2


def greet():
    sp, z, core = tp_place()
    tp = z * 2 + core
    barrier = pltpu.get_barrier_semaphore()
    peers = [(sp, ((z + 1) % 8) * 2 + core), (sp, ((z + 7) % 8) * 2 + core), (sp, tp + 1 - 2 * core)]
    peers += [((sp + delta) % 16, tp) for delta in range(1, 16)]
    for peer in peers:
        pl.semaphore_signal(barrier, inc=1, device_id=peer, device_id_type=MESH)
    return len(peers)


class Exchange:
    def __init__(self, pbuf, other, stage, landed, pair_send, pair_recv, ring_send, ring_recv):
        self.sp, self.z, self.core = tp_place()
        self.pbuf, self.other, self.stage, self.landed = pbuf, other, stage, landed
        self.pair_sems, self.ring_sems = (pair_send, pair_recv), (ring_send, ring_recv)
        self.rows, self.wide = pbuf.shape[1] // 2, pbuf.shape[2] // PIECES

    def chip(self, offset):
        return (self.z + offset + 8) % 8

    def pair_copy(self, offset):
        chip = self.chip(offset)
        return pltpu.make_async_remote_copy(
            src_ref=self.pbuf.at[chip * 2 + 1 - self.core],
            dst_ref=self.other.at[chip],
            send_sem=self.pair_sems[0].at[offset + 3],
            recv_sem=self.pair_sems[1].at[offset + 3],
            device_id=(self.sp, self.z * 2 + 1 - self.core),
            device_id_type=MESH,
        )

    def ring_copy(self, way, half, distance, piece):
        number = ((way * 2 + half) * 4 + distance - 1) * PIECES + piece
        columns = pl.ds(piece * self.wide, self.wide)
        return pltpu.make_async_remote_copy(
            src_ref=self.stage.at[way, half, distance - 1, :, columns],
            dst_ref=self.landed.at[way, half, distance - 1, :, columns],
            send_sem=self.ring_sems[0].at[number],
            recv_sem=self.ring_sems[1].at[number],
            device_id=(self.sp, self.chip(1 - 2 * way) * 2 + self.core),
            device_id_type=MESH,
        )

    def mine(self, offset, half, columns=slice(None)):
        chip = self.chip(offset)
        rows = slice(half * self.rows, (half + 1) * self.rows)
        own = self.pbuf[chip * 2 + self.core, rows, columns].astype(jnp.float32)
        return own + self.other[chip, rows, columns].astype(jnp.float32)

    def send(self, way, half, distance):
        offset = distance * (1 - 2 * way)
        for piece in range(PIECES):
            columns = slice(piece * self.wide, (piece + 1) * self.wide)
            total = self.mine(4 if distance == 4 else offset, half, columns)
            if distance < (4 if half == way else 3):
                self.ring_copy(way, half, distance + 1, piece).wait_recv()
                total = total + self.landed[way, half, distance, :, columns].astype(jnp.float32)
            self.stage[way, half, distance - 1, :, columns] = total.astype(jnp.bfloat16)
            self.ring_copy(way, half, distance, piece).start()

    def last(self, half):
        total = self.mine(0, half)
        for way in range(2):
            for piece in range(PIECES):
                self.ring_copy(way, half, 1, piece).wait_recv()
            total = total + self.landed[way, half, 0].astype(jnp.float32)
        return total

    def finish(self):
        for offset in range(-3, 5):
            self.pair_copy(offset).wait_send()
        for way in range(2):
            for half in range(2):
                for distance in range(1, 5 if half == way else 4):
                    for piece in range(PIECES):
                        self.ring_copy(way, half, distance, piece).wait_send()


def exchange_scratch(rows, width):
    return [
        pltpu.VMEM((16, rows, width), jnp.bfloat16),
        pltpu.VMEM((8, rows, width), jnp.bfloat16),
        pltpu.VMEM((2, 2, 4, rows // 2, width), jnp.bfloat16),
        pltpu.VMEM((2, 2, 4, rows // 2, width), jnp.bfloat16),
        pltpu.SemaphoreType.DMA((8,)),
        pltpu.SemaphoreType.DMA((8,)),
        pltpu.SemaphoreType.DMA((16 * PIECES,)),
        pltpu.SemaphoreType.DMA((16 * PIECES,)),
    ]


SLAB = 8


def slab_copy(slabs, landing, delta, send_sem, recv_sem, arriving=False):
    sp, tp = lax.axis_index("sp"), lax.axis_index("tp")
    there = (sp + delta) % 16
    return pltpu.make_async_remote_copy(
        src_ref=slabs.at[there],
        dst_ref=landing.at[(sp + 16 - delta) % 16 if arriving else sp],
        send_sem=send_sem.at[delta],
        recv_sem=recv_sem.at[delta],
        device_id=(there, tp),
        device_id_type=MESH,
    )


def chosen_slots(ids_ref):
    tokens = ids_ref.shape[1]
    expert = lax.broadcasted_iota(jnp.int32, (16, tokens), 0)
    named = [(expert == ids_ref[r : r + 1, :]).astype(jnp.float32) for r in range(2)]
    earlier = lax.broadcasted_iota(jnp.int32, (tokens, tokens), 0)
    earlier = (earlier < lax.broadcasted_iota(jnp.int32, (tokens, tokens), 1)).astype(jnp.bfloat16)
    before = dot32((named[0] + named[1]).astype(jnp.bfloat16), earlier)
    slots = lax.broadcasted_iota(jnp.int32, (16 * SLAB, tokens), 0)
    result = []
    for r in range(2):
        rank = jnp.sum(named[r] * before, axis=0, keepdims=True).astype(jnp.int32)
        result.append((slots == ids_ref[r : r + 1, :] * SLAB + rank).astype(jnp.bfloat16))
    return result


def packing(rows, capacity):
    shape = (rows, rows // capacity * SLAB)
    row = lax.broadcasted_iota(jnp.int32, shape, 0)
    column = lax.broadcasted_iota(jnp.int32, shape, 1)
    used = column % SLAB < capacity
    return (used & (row == column // SLAB * capacity + column % SLAB)).astype(jnp.bfloat16)


def unpacking(rows, capacity):
    shape = (rows // capacity * SLAB, rows)
    row = lax.broadcasted_iota(jnp.int32, shape, 0)
    column = lax.broadcasted_iota(jnp.int32, shape, 1)
    used = row % SLAB < capacity
    return (used & (column == row // SLAB * capacity + row % SLAB)).astype(jnp.bfloat16)


def experts_part(
    heads_ref, proj_a_ref, proj_b_ref, resid_ref, gain_ref, ids_ref, weights_ref,
    gate_hbm, up_hbm, down_hbm, out_ref,
    mixed, slabs, landing, returned, back, go_send, go_recv, back_send, back_recv,
    xbuf, gate, up, down, w_sem, ag_send, ag_recv, share_send, share_recv, *exchange,
):
    sp, z, core = tp_place()
    px = Exchange(*exchange[:8])
    ex = Exchange(*exchange[8:])
    width = mixed.shape[1]
    pbuf = ex.pbuf
    for first in range(0, width, 512):
        cols = slice(first, first + 512)
        term = dot32(heads_ref[:, 0:128], proj_a_ref[:, cols])
        term = term + dot32(heads_ref[:, 128:192], proj_b_ref[:, cols])
        px.pbuf[:, :, cols] = term.astype(jnp.bfloat16).reshape(16, 32, 512)
    for offset in (4, 3, -3, 2, -2, 1, -1, 0):
        px.pair_copy(offset).start()
    chosen = chosen_slots(ids_ref)
    px.pair_copy(4).wait_recv()
    px.send(0, 0, 4)
    px.send(1, 1, 4)
    for distance in (3, 2, 1):
        px.pair_copy(distance).wait_recv()
        px.pair_copy(-distance).wait_recv()
        if distance == 3:
            px.send(0, 1, 3)
            px.send(1, 0, 3)
        px.send(0, 0, distance)
        px.send(1, 1, distance)
        if distance < 3:
            px.send(0, 1, distance)
            px.send(1, 0, distance)
    px.pair_copy(0).wait_recv()
    for half in range(2):
        rows = slice(half * 16, half * 16 + 16)
        mixed[rows, :] = resid_ref[rows, :].astype(jnp.float32) + px.last(half)
    normed = rms_scaled(mixed[...], gain_ref[...]).astype(jnp.bfloat16)
    outgoing = dot32(chosen[0] + chosen[1], normed).astype(jnp.bfloat16)
    slabs[...] = outgoing.reshape(16, SLAB, width)
    for delta in range(1, 16):
        slab_copy(slabs, landing, delta, go_send, go_recv).start()
    landing[sp] = slabs[sp]
    for delta in range(1, 16):
        slab_copy(slabs, landing, delta, go_send, go_recv, arriving=True).wait_recv()
    count = xbuf.shape[1]
    capacity = count // 16
    arrived = landing[...].reshape(16 * SLAB, width)
    xbuf[z * 2 + core] = dot32(packing(count, capacity), arrived).astype(jnp.bfloat16)
    part = count // 2

    def shard(offset, half):
        chip = ex.chip(offset)
        return xbuf.at[chip * 2 + core, pl.ds(half * part, part)]

    def ag_copy(way, half, distance, arriving=False):
        sign = 1 - 2 * way
        away = distance + 1 if arriving else distance
        offset = 4 if away == 4 else -sign * away
        number = way * 8 + half * 4 + distance
        return pltpu.make_async_remote_copy(
            src_ref=shard(offset, half),
            dst_ref=shard(offset, half),
            send_sem=ag_send.at[number],
            recv_sem=ag_recv.at[number],
            device_id=(sp, ex.chip(sign) * 2 + core),
            device_id_type=MESH,
        )

    def share_copy(offset, half, arriving=False):
        chip = ex.chip(offset)
        there = xbuf.at[chip * 2 + (1 - core if arriving else core), pl.ds(half * part, part)]
        number = (offset + 3) * 2 + half
        return pltpu.make_async_remote_copy(
            src_ref=there,
            dst_ref=there,
            send_sem=share_send.at[number],
            recv_sem=share_recv.at[number],
            device_id=(sp, z * 2 + 1 - core),
            device_id_type=MESH,
        )

    def came(way, half, distance):
        ag_copy(way, half, distance - 1, arriving=True).wait_recv()
        if distance < (4 if half == way else 3):
            ag_copy(way, half, distance).start()
        offset = 4 if distance == 4 else -distance * (1 - 2 * way)
        share_copy(offset, half).start()

    def feed(offset):
        for half in range(2):
            share_copy(offset, half, arriving=True).wait_recv()

    def experts(first, count):
        def step(number, carry):
            chip = ex.chip(first - 2 * first * number)
            piece = xbuf[pl.ds(chip * 2, 2)].reshape(4 * part, xbuf.shape[2])
            gated = dot32(piece, gate[0])
            upward = dot32(piece, up[0])
            hidden = (jax.nn.silu(gated) * upward).astype(jnp.bfloat16)
            for begin in range(0, xbuf.shape[2], 512):
                cols = slice(begin, begin + 512)
                term = dot32(hidden, down[0, :, cols]).astype(jnp.bfloat16)
                pbuf[pl.ds(chip * 2, 2), :, cols] = term.reshape(2, 2 * part, 512)
            return carry

        lax.fori_loop(0, count, step, 0)

    for way in range(2):
        ag_copy(way, way, 0).start()
        ag_copy(way, 1 - way, 0).start()
    for half in range(2):
        share_copy(0, half).start()
    for distance in (1, 2, 3):
        came(0, 0, distance)
        came(1, 1, distance)
        came(0, 1, distance)
        came(1, 0, distance)
        if distance == 1:
            for load in weight_loads(gate_hbm, up_hbm, down_hbm, gate, up, down, w_sem):
                load.wait()
            feed(0)
            experts(0, 1)
            ex.pair_copy(0).start()
        else:
            feed(1 - distance)
            feed(distance - 1)
            experts(distance - 1, 2)
            ex.pair_copy(1 - distance).start()
            ex.pair_copy(distance - 1).start()
    feed(-3)
    feed(3)
    experts(3, 2)
    ex.pair_copy(-3).start()
    ex.pair_copy(3).start()
    came(0, 0, 4)
    came(1, 1, 4)
    ex.pair_copy(3).wait_recv()
    ex.send(0, 1, 3)
    ex.pair_copy(-3).wait_recv()
    ex.send(1, 0, 3)
    feed(4)
    experts(4, 1)
    ex.pair_copy(4).start()
    for offset in (2, -2, 1, -1, 0, 4):
        ex.pair_copy(offset).wait_recv()
    ex.send(0, 0, 4)
    ex.send(1, 1, 4)
    for distance in (3, 2, 1):
        if distance < 3:
            ex.send(0, 1, distance)
            ex.send(1, 0, distance)
        ex.send(0, 0, distance)
        ex.send(1, 1, distance)
    widen = unpacking(part, capacity)
    for half in range(2):
        summed = ex.last(half).astype(jnp.bfloat16)
        spread = dot32(widen, summed).astype(jnp.bfloat16)
        returned[half * 8 : half * 8 + 8] = spread.reshape(8, SLAB, width)
    for delta in range(1, 16):
        slab_copy(returned, back, delta, back_send, back_recv).start()
    back[sp] = returned[sp]
    tokens = mixed.shape[0]
    row = lax.broadcasted_iota(jnp.int32, (tokens, tokens), 0)
    same = row == lax.broadcasted_iota(jnp.int32, (tokens, tokens), 1)
    picks = [jnp.transpose(c.astype(jnp.float32)).astype(jnp.bfloat16) for c in chosen]
    factors = [
        jnp.sum(jnp.where(same, weights_ref[r : r + 1, :], 0.0), axis=1, keepdims=True)
        for r in range(2)
    ]
    for delta in range(1, 16):
        slab_copy(returned, back, delta, back_send, back_recv, arriving=True).wait_recv()
    rows = back[...].reshape(16 * SLAB, width)
    added = factors[0] * dot32(picks[0], rows) + factors[1] * dot32(picks[1], rows)
    out_ref[...] = (mixed[...] + added).astype(jnp.bfloat16)
    for delta in range(1, 16):
        slab_copy(slabs, landing, delta, go_send, go_recv).wait_send()
        slab_copy(returned, back, delta, back_send, back_recv).wait_send()
    px.finish()
    ex.finish()
    for way in range(2):
        for half in range(2):
            for distance in range(4 if half == way else 3):
                ag_copy(way, half, distance).wait_send()
    for offset in range(-3, 5):
        for half in range(2):
            share_copy(offset, half).wait_send()


def weight_loads(gate_hbm, up_hbm, down_hbm, gate, up, down, w_sem):
    pairs = ((gate_hbm, gate), (up_hbm, up), (down_hbm, down))
    return [pltpu.make_async_copy(a, b, w_sem.at[i]) for i, (a, b) in enumerate(pairs)]


ATTENTION_INPUTS, ATTENTION_SCRATCH = 10, 14


def whole_kernel(*refs):
    inputs, (out_ref, heads), scratch = refs[:19], refs[19:21], refs[21:]
    own, rest = scratch[:ATTENTION_SCRATCH], scratch[ATTENTION_SCRATCH:]
    for load in weight_loads(*inputs[16:19], *rest[10:14]):
        load.start()
    finish = attention_part(*inputs[:ATTENTION_INPUTS], heads, *own)
    experts_part(heads, *inputs[ATTENTION_INPUTS:], out_ref, *rest)
    finish()


def per_device(
    resid,
    query_a,
    key_a,
    value_a,
    query_b,
    key_b,
    value_b,
    mix_a,
    mix_b,
    head_gain_a,
    head_gain_b,
    proj_a,
    proj_b,
    norm_gain,
    route_ids,
    route_weights,
    expert_gate,
    expert_up,
    expert_down,
):
    tokens, width = resid.shape
    rows = query_a.shape[0]
    half = rows // 2
    count = 3 * route_ids.shape[1] * tokens // 2
    vmem = pl.BlockSpec(memory_space=pltpu.VMEM)
    smem = pl.BlockSpec(memory_space=pltpu.SMEM)
    anywhere = pl.BlockSpec(memory_space=pl.ANY)
    attention_scratch = [
        pltpu.VMEM((16, 2, half, 384), jnp.bfloat16),
        pltpu.VMEM((4, 128, half), jnp.bfloat16),
        pltpu.VMEM((4, 64, half), jnp.bfloat16),
        pltpu.VMEM((2, half, 64), jnp.bfloat16),
        pltpu.VMEM((rows, half), jnp.float32),
        pltpu.VMEM((rows, half), jnp.float32),
        pltpu.VMEM((rows, half), jnp.bfloat16),
        pltpu.VMEM((rows, half), jnp.bfloat16),
        pltpu.VMEM((4, 128, half), jnp.float32),
        pltpu.VMEM((4, 64, half), jnp.float32),
        pltpu.VMEM((8, 1, half), jnp.float32),
        pltpu.VMEM((8, 8, half), jnp.float32),
        pltpu.SemaphoreType.DMA((40,)),
        pltpu.SemaphoreType.DMA((40,)),
    ]
    experts_scratch = [
        pltpu.VMEM((tokens, width), jnp.float32),
        *[pltpu.VMEM((16, SLAB, width), jnp.bfloat16)] * 4,
        *[pltpu.SemaphoreType.DMA((16,))] * 4,
        pltpu.VMEM((16, count, width), jnp.bfloat16),
        pltpu.VMEM(expert_gate.shape, expert_gate.dtype),
        pltpu.VMEM(expert_up.shape, expert_up.dtype),
        pltpu.VMEM(expert_down.shape, expert_down.dtype),
        pltpu.SemaphoreType.DMA((3,)),
        *[pltpu.SemaphoreType.DMA((16,))] * 4,
        *exchange_scratch(tokens, width),
        *exchange_scratch(count, width),
    ]
    return pl.pallas_call(
        whole_kernel,
        out_shape=jax.ShapeDtypeStruct((tokens, width), jnp.bfloat16),
        in_specs=[vmem] * 6 + [smem] * 2 + [vmem] * 8 + [anywhere] * 3,
        out_specs=vmem,
        scratch_shapes=[pltpu.VMEM((rows, 192), jnp.bfloat16), *attention_scratch, *experts_scratch],
        compiler_params=pltpu.CompilerParams(
            collective_id=0, has_side_effects=True, vmem_limit_bytes=60 * 1024 * 1024
        ),
    )(
        query_a[:, 0, :], query_b[:, 0, :].T, key_a[:, 0, :], value_a[:, 0, :],
        key_b[:, 0, :].T, value_b[:, 0, :].T,
        mix_a, mix_b, head_gain_a[None, :], head_gain_b[None, :],
        proj_a, proj_b, resid, norm_gain[None, :], route_ids.T, route_weights.T,
        expert_gate, expert_up, expert_down,
    )


def solution(mesh):
    placed = (
        P(("sp", "tp"), None),
        P("sp", "tp", None),
        P("sp", "tp", None),
        P("sp", "tp", None),
        P("sp", "tp", None),
        P("sp", "tp", None),
        P("sp", "tp", None),
        P("tp"),
        P("tp"),
        P(),
        P(),
        P("tp", None),
        P("tp", None),
        P(),
        P(("sp", "tp"), None),
        P(("sp", "tp"), None),
        P("sp", None, "tp"),
        P("sp", None, "tp"),
        P("sp", "tp", None),
    )
    return jax.shard_map(
        per_device, mesh=mesh, in_specs=placed, out_specs=P(("sp", "tp"), None), check_vma=False
    )
```

```python
import math

import jax
import jax.numpy as jnp
from jax import lax
from jax.experimental import pallas as pl
from jax.experimental.pallas import tpu as pltpu
from jax.sharding import PartitionSpec as P

EPS = 1e-06
NEG = -1e30
HEAD_SCALE = 1.0 - (0.8 - 0.6 * math.exp(-0.3))


def rms_scaled(values, gain):
    return values * lax.rsqrt(jnp.mean(values * values, axis=-1, keepdims=True) + EPS) * gain


MESH = pl.DeviceIdType.MESH
LOG2E = 1.4426950408889634
PART = 128
CHUNK = 64
PIECES = 4


def dot32(a, b):
    return jnp.dot(a, b, preferred_element_type=jnp.float32)


def attention_part(
    qa_ref, qb_ref, ka_ref, va_ref, kb_ref, vb_ref, mix_a_ref, mix_b_ref, gain_a_ref, gain_b_ref,
    out_ref,
    buf, qta, qtb, k_b, s_0, s_1, s_2, s_3, p_0, p_1, p_2, p_3, acc_a, acc_b, m_ref, l_ref,
    send_sem, recv_sem,
):
    s_refs, p_refs = (s_0, s_1, s_2, s_3), (p_0, p_1, p_2, p_3)
    place = lax.axis_index("sp")
    tp = lax.axis_index("tp")
    y, x = place // 4, place % 4
    half = buf.shape[2]

    def at(ox, oy):
        return ((y + oy + 4) % 4) * 4 + (x + ox + 4) % 4

    def spot(h, df, dg):
        return at(df, dg) if h == 0 else at(dg, df)

    peers = greet()

    va_t = jnp.transpose(va_ref[...])
    for h in range(2):
        cols = slice(h * half, (h + 1) * half)
        buf[place, h, :, 0:128] = ka_ref[cols, :]
        buf[place, h, 0:128, 128:384] = va_t[:, cols]
        buf[place, h, 128:192, 128:384] = kb_ref[:, cols]
        buf[place, h, 192:256, 128:384] = vb_ref[:, cols]

    pl.semaphore_wait(pltpu.get_barrier_semaphore(), peers)

    def region(h, df, dg, part):
        ref = buf.at[spot(h, df, dg), h]
        return ref if part is None else ref.at[pl.ds(part * PART, PART)]

    def copy(h, number, df, dg, part, to_f, to_g):
        ref = region(h, df, dg, part)
        return pltpu.make_async_remote_copy(
            src_ref=ref,
            dst_ref=ref,
            send_sem=send_sem.at[h * 20 + number],
            recv_sem=recv_sem.at[h * 20 + number],
            device_id=(spot(h, to_f, to_g), tp),
            device_id_type=MESH,
        )

    moves = {
        0: (0, 0, None, 1, 0), 1: (0, 0, None, -1, 0),
        2: (0, 0, None, 0, 1), 3: (0, 0, None, 0, -1),
        4: (-1, 0, 0, 1, 0), 5: (1, 0, 1, -1, 0),
        6: (-1, 0, None, 0, 1), 7: (-1, 0, None, 0, -1),
        8: (1, 0, None, 0, 1), 9: (1, 0, None, 0, -1),
        10: (2, 0, None, 0, 1), 11: (2, 0, None, 0, -1),
        12: (0, -1, 0, 0, 1), 13: (0, 1, 1, 0, -1),
        14: (-1, -1, 0, 0, 1), 15: (-1, 1, 1, 0, -1),
        16: (1, -1, 0, 0, 1), 17: (1, 1, 1, 0, -1),
        18: (2, -1, 0, 0, 1), 19: (2, 1, 1, 0, -1),
    }

    def start(*numbers):
        for number in numbers:
            for h in range(2):
                copy(h, number, *moves[number]).start()

    def arrive(number, *then):
        df, dg, part, to_f, to_g = moves[number]
        for h in range(2):
            copy(h, number, df - to_f, dg - to_g, part, to_f, to_g).wait_recv()
            for follow in then:
                copy(h, follow, *moves[follow]).start()

    start(0, 1, 2, 3)

    qa_t = jnp.transpose(qa_ref[...])
    zero_a = jnp.zeros((64, half), jnp.bfloat16)
    zero_b = jnp.zeros((32, half), jnp.bfloat16)
    for h in range(2):
        cols = slice(h * half, (h + 1) * half)
        qta[h, 0:64, :] = qa_t[0:64, cols]
        qta[h, 64:128, :] = zero_a
        qta[2 + h, 0:64, :] = zero_a
        qta[2 + h, 64:128, :] = qa_t[64:128, cols]
        qtb[h, 0:32, :] = qb_ref[0:32, cols]
        qtb[h, 32:64, :] = zero_b
        qtb[2 + h, 0:32, :] = zero_b
        qtb[2 + h, 32:64, :] = qb_ref[32:64, cols]
    acc_a[...] = jnp.zeros_like(acc_a)
    acc_b[...] = jnp.zeros_like(acc_b)
    m_ref[...] = jnp.full_like(m_ref, NEG)
    l_ref[...] = jnp.zeros_like(l_ref)

    def score(number, source, offsets):
        index, group, place_in = number // 2, number % 2, number % 2
        top = None
        for h in range(2):
            keys = k_b[h] if group else buf[source, h, :, 0:128]
            found = dot32(keys, qtb[index] if group else qta[index])
            if offsets is not None:
                query_pos = (index % 2) * half + lax.broadcasted_iota(jnp.int32, (half, half), 1)
                key_pos = offsets[h] + lax.broadcasted_iota(jnp.int32, (half, half), 0)
                found = jnp.where(key_pos <= query_pos, found, NEG)
            s_refs[number % 4][h * half : (h + 1) * half, :] = found
            most = jnp.max(found.reshape(half // 8, 8, half), axis=0)
            top = most if top is None else jnp.maximum(top, most)
        return jnp.max(top, axis=0, keepdims=True)

    def soften(number, top):
        index, group = number // 2, number % 2
        slot, factor = index + 4 * group, (LOG2E / math.sqrt(32.0) if group else LOG2E / 8.0)
        old = m_ref[slot]
        fresh = jnp.maximum(old, top)
        scale = jnp.exp2((old - fresh) * factor)
        m_ref[slot] = fresh
        sums = l_ref[slot] * scale
        for first in range(0, 2 * half, CHUNK):
            rows = slice(first, first + CHUNK)
            weights = jnp.exp2((s_refs[number % 4][rows, :] - fresh) * factor)
            sums = sums + jnp.sum(weights.reshape(CHUNK // 8, 8, half), axis=0)
            p_refs[number % 4][rows, :] = weights.astype(jnp.bfloat16)
        l_ref[slot] = sums
        return scale

    def gather(number, source, scale):
        index, group = number // 2, number % 2
        acc, rows = (acc_b, slice(192, 256)) if group else (acc_a, slice(0, 128))
        added = dot32(buf[source, 0, rows, 128:384], p_refs[number % 4][0:half, :])
        added = added + dot32(buf[source, 1, rows, 128:384], p_refs[number % 4][half : 2 * half, :])
        acc[index] = acc[index] * scale + added

    def block(source, offsets):
        for h in range(2):
            k_b[h] = jnp.transpose(buf[source, h, 128:192, 128:384])
        tops = [score(number, source, offsets) for number in range(2)]
        for number in range(8):
            if number + 2 < 8:
                tops.append(score(number + 2, source, offsets))
            gather(number, source, soften(number, tops[number]))

    plan = (
        ((-1, 0), ()), ((0, -1), (4, 5)), ((1, 0), ()), ((0, 1), (6, 7)), ((-1, -1), ()),
        ((2, 0), (12, 13)), ((0, 2), (8, 9)), ((1, -1), ()), ((-1, 1), ()), ((1, 1), ()),
        ((2, -1), (10, 11, 14, 15)), ((-1, 2), (16, 17)), ((2, 1), ()), ((1, 2), (18, 19)),
        ((2, 2), ()),
    )
    follow = {5: (10, 11), 6: (14,), 7: (15,), 8: (16,), 9: (17,), 10: (18,), 11: (19,)}

    def step(number, carry):
        ox, oy = jnp.int32(0), jnp.int32(0)
        for which, ((dx, dy), events) in enumerate(plan):
            ox = jnp.where(number == which, dx, ox)
            oy = jnp.where(number == which, dy, oy)
            if events:

                @pl.when(number == which)
                def _(events=events):
                    for event in events:
                        arrive(event, *follow.get(event, ()))

        source = at(ox, oy)

        @pl.when(source < place)
        def _():
            block(source, None)

        return carry

    block(place, (0, half))
    arrive(0, 4, 6, 7)
    arrive(1, 5)
    arrive(2, 12)
    arrive(3, 13, 8, 9)
    lax.fori_loop(0, len(plan), step, 0)

    for h in range(2):
        for acc, base, mix, gain, first in (
            (acc_a, 0, mix_a_ref, gain_a_ref, 0), (acc_b, 4, mix_b_ref, gain_b_ref, 128),
        ):
            one = acc[h] / jnp.sum(l_ref[base + h], axis=0, keepdims=True)
            two = acc[2 + h] / jnp.sum(l_ref[base + 2 + h], axis=0, keepdims=True)
            mixed = one - mix[0] * two
            mixed = mixed * lax.rsqrt(jnp.mean(mixed * mixed, axis=0, keepdims=True) + EPS)
            rows = jnp.transpose(mixed) * gain[...] * HEAD_SCALE
            out_ref[h * half : (h + 1) * half, first : first + rows.shape[1]] = rows.astype(
                jnp.bfloat16
            )

    def finish():
        for number in range(20):
            for h in range(2):
                copy(h, number, *moves[number]).wait_send()

    return finish


def tp_place():
    tp = lax.axis_index("tp")
    return lax.axis_index("sp"), tp // 2, tp % 2


def greet():
    sp, z, core = tp_place()
    tp = z * 2 + core
    barrier = pltpu.get_barrier_semaphore()
    peers = [(sp, ((z + 1) % 8) * 2 + core), (sp, ((z + 7) % 8) * 2 + core), (sp, tp + 1 - 2 * core)]
    peers += [((sp + delta) % 16, tp) for delta in range(1, 16)]
    for peer in peers:
        pl.semaphore_signal(barrier, inc=1, device_id=peer, device_id_type=MESH)
    return len(peers)


class Exchange:
    def __init__(self, pbuf, other, stage, landed, pair_send, pair_recv, ring_send, ring_recv):
        self.sp, self.z, self.core = tp_place()
        self.pbuf, self.other, self.stage, self.landed = pbuf, other, stage, landed
        self.pair_sems, self.ring_sems = (pair_send, pair_recv), (ring_send, ring_recv)
        self.rows, self.wide = pbuf.shape[1] // 2, pbuf.shape[2] // PIECES

    def chip(self, offset):
        return (self.z + offset + 8) % 8

    def pair_copy(self, offset, half):
        chip = self.chip(offset)
        rows = pl.ds(half * self.rows, self.rows)
        number = (offset + 3) * 2 + half
        return pltpu.make_async_remote_copy(
            src_ref=self.pbuf.at[chip * 2 + 1 - self.core, rows],
            dst_ref=self.other.at[chip, rows],
            send_sem=self.pair_sems[0].at[number],
            recv_sem=self.pair_sems[1].at[number],
            device_id=(self.sp, self.z * 2 + 1 - self.core),
            device_id_type=MESH,
        )

    def give(self, *offsets):
        for offset in offsets:
            for half in range(2):
                self.pair_copy(offset, half).start()

    def take(self, *offsets):
        for offset in offsets:
            for half in range(2):
                self.pair_copy(offset, half).wait_recv()

    def ring_copy(self, way, half, distance, piece):
        number = ((way * 2 + half) * 4 + distance - 1) * PIECES + piece
        columns = pl.ds(piece * self.wide, self.wide)
        return pltpu.make_async_remote_copy(
            src_ref=self.stage.at[way, half, distance - 1, :, columns],
            dst_ref=self.landed.at[way, half, distance - 1, :, columns],
            send_sem=self.ring_sems[0].at[number],
            recv_sem=self.ring_sems[1].at[number],
            device_id=(self.sp, self.chip(1 - 2 * way) * 2 + self.core),
            device_id_type=MESH,
        )

    def mine(self, offset, half, columns=slice(None)):
        chip = self.chip(offset)
        rows = slice(half * self.rows, (half + 1) * self.rows)
        own = self.pbuf[chip * 2 + self.core, rows, columns].astype(jnp.float32)
        return own + self.other[chip, rows, columns].astype(jnp.float32)

    def send(self, way, half, distance):
        offset = distance * (1 - 2 * way)
        for piece in range(PIECES):
            columns = slice(piece * self.wide, (piece + 1) * self.wide)
            total = self.mine(4 if distance == 4 else offset, half, columns)
            if distance < (4 if half == way else 3):
                self.ring_copy(way, half, distance + 1, piece).wait_recv()
                total = total + self.landed[way, half, distance, :, columns].astype(jnp.float32)
            self.stage[way, half, distance - 1, :, columns] = total.astype(jnp.bfloat16)
            self.ring_copy(way, half, distance, piece).start()

    def last(self, half):
        total = self.mine(0, half)
        for way in range(2):
            for piece in range(PIECES):
                self.ring_copy(way, half, 1, piece).wait_recv()
            total = total + self.landed[way, half, 0].astype(jnp.float32)
        return total

    def finish(self):
        for offset in range(-3, 5):
            for half in range(2):
                self.pair_copy(offset, half).wait_send()
        for way in range(2):
            for half in range(2):
                for distance in range(1, 5 if half == way else 4):
                    for piece in range(PIECES):
                        self.ring_copy(way, half, distance, piece).wait_send()


def exchange_scratch(rows, width):
    return [
        pltpu.VMEM((16, rows, width), jnp.bfloat16),
        pltpu.VMEM((8, rows, width), jnp.bfloat16),
        pltpu.VMEM((2, 2, 4, rows // 2, width), jnp.bfloat16),
        pltpu.VMEM((2, 2, 4, rows // 2, width), jnp.bfloat16),
        pltpu.SemaphoreType.DMA((16,)),
        pltpu.SemaphoreType.DMA((16,)),
        pltpu.SemaphoreType.DMA((16 * PIECES,)),
        pltpu.SemaphoreType.DMA((16 * PIECES,)),
    ]


SLAB = 8


def slab_copy(slabs, landing, delta, send_sem, recv_sem, arriving=False):
    sp, tp = lax.axis_index("sp"), lax.axis_index("tp")
    there = (sp + delta) % 16
    return pltpu.make_async_remote_copy(
        src_ref=slabs.at[there],
        dst_ref=landing.at[(sp + 16 - delta) % 16 if arriving else sp],
        send_sem=send_sem.at[delta],
        recv_sem=recv_sem.at[delta],
        device_id=(there, tp),
        device_id_type=MESH,
    )


def chosen_slots(ids_ref):
    tokens = ids_ref.shape[1]
    expert = lax.broadcasted_iota(jnp.int32, (16, tokens), 0)
    named = [(expert == ids_ref[r : r + 1, :]).astype(jnp.float32) for r in range(2)]
    earlier = lax.broadcasted_iota(jnp.int32, (tokens, tokens), 0)
    earlier = (earlier < lax.broadcasted_iota(jnp.int32, (tokens, tokens), 1)).astype(jnp.bfloat16)
    before = dot32((named[0] + named[1]).astype(jnp.bfloat16), earlier)
    slots = lax.broadcasted_iota(jnp.int32, (16 * SLAB, tokens), 0)
    result = []
    for r in range(2):
        rank = jnp.sum(named[r] * before, axis=0, keepdims=True).astype(jnp.int32)
        result.append((slots == ids_ref[r : r + 1, :] * SLAB + rank).astype(jnp.bfloat16))
    return result


def packing(rows, capacity):
    shape = (rows, rows // capacity * SLAB)
    row = lax.broadcasted_iota(jnp.int32, shape, 0)
    column = lax.broadcasted_iota(jnp.int32, shape, 1)
    used = column % SLAB < capacity
    return (used & (row == column // SLAB * capacity + column % SLAB)).astype(jnp.bfloat16)


def unpacking(rows, capacity):
    shape = (rows // capacity * SLAB, rows)
    row = lax.broadcasted_iota(jnp.int32, shape, 0)
    column = lax.broadcasted_iota(jnp.int32, shape, 1)
    used = row % SLAB < capacity
    return (used & (column == row // SLAB * capacity + row % SLAB)).astype(jnp.bfloat16)


def experts_part(
    heads_ref, proj_a_ref, proj_b_ref, resid_ref, gain_ref, ids_ref, weights_ref,
    gate_hbm, up_hbm, down_hbm, out_ref,
    mixed, slabs, landing, returned, back, go_send, go_recv, back_send, back_recv,
    xbuf, gate, up, down, w_sem, ag_send, ag_recv, share_send, share_recv, *exchange,
):
    sp, z, core = tp_place()
    px = Exchange(*exchange[:8])
    ex = Exchange(*exchange[8:])
    width = mixed.shape[1]
    pbuf = ex.pbuf
    for first in range(0, width, 512):
        cols = slice(first, first + 512)
        term = dot32(heads_ref[:, 0:128], proj_a_ref[:, cols])
        term = term + dot32(heads_ref[:, 128:192], proj_b_ref[:, cols])
        px.pbuf[:, :, cols] = term.astype(jnp.bfloat16).reshape(16, 32, 512)
    px.give(4, 3, -3, 2, -2, 1, -1, 0)
    chosen = chosen_slots(ids_ref)
    px.take(4)
    px.send(0, 0, 4)
    px.send(1, 1, 4)
    for distance in (3, 2, 1):
        px.take(distance, -distance)
        if distance == 3:
            px.send(0, 1, 3)
            px.send(1, 0, 3)
        px.send(0, 0, distance)
        px.send(1, 1, distance)
        if distance < 3:
            px.send(0, 1, distance)
            px.send(1, 0, distance)
    px.take(0)
    for half in range(2):
        rows = slice(half * 16, half * 16 + 16)
        mixed[rows, :] = resid_ref[rows, :].astype(jnp.float32) + px.last(half)
    normed = rms_scaled(mixed[...], gain_ref[...]).astype(jnp.bfloat16)
    outgoing = dot32(chosen[0] + chosen[1], normed).astype(jnp.bfloat16)
    slabs[...] = outgoing.reshape(16, SLAB, width)
    for delta in range(1, 16):
        slab_copy(slabs, landing, delta, go_send, go_recv).start()
    landing[sp] = slabs[sp]
    for delta in range(1, 16):
        slab_copy(slabs, landing, delta, go_send, go_recv, arriving=True).wait_recv()
    count = xbuf.shape[1]
    capacity = count // 16
    arrived = landing[...].reshape(16 * SLAB, width)
    xbuf[z * 2 + core] = dot32(packing(count, capacity), arrived).astype(jnp.bfloat16)
    part = count // 2

    def shard(offset, half):
        chip = ex.chip(offset)
        return xbuf.at[chip * 2 + core, pl.ds(half * part, part)]

    def ag_copy(way, half, distance, arriving=False):
        sign = 1 - 2 * way
        away = distance + 1 if arriving else distance
        offset = 4 if away == 4 else -sign * away
        number = way * 8 + half * 4 + distance
        return pltpu.make_async_remote_copy(
            src_ref=shard(offset, half),
            dst_ref=shard(offset, half),
            send_sem=ag_send.at[number],
            recv_sem=ag_recv.at[number],
            device_id=(sp, ex.chip(sign) * 2 + core),
            device_id_type=MESH,
        )

    def share_copy(offset, half, arriving=False):
        chip = ex.chip(offset)
        there = xbuf.at[chip * 2 + (1 - core if arriving else core), pl.ds(half * part, part)]
        number = (offset + 3) * 2 + half
        return pltpu.make_async_remote_copy(
            src_ref=there,
            dst_ref=there,
            send_sem=share_send.at[number],
            recv_sem=share_recv.at[number],
            device_id=(sp, z * 2 + 1 - core),
            device_id_type=MESH,
        )

    def came(way, half, distance):
        ag_copy(way, half, distance - 1, arriving=True).wait_recv()
        if distance < (4 if half == way else 3):
            ag_copy(way, half, distance).start()
        offset = 4 if distance == 4 else -distance * (1 - 2 * way)
        share_copy(offset, half).start()

    def feed(offset):
        for half in range(2):
            share_copy(offset, half, arriving=True).wait_recv()

    def feed_half(offset, half):
        share_copy(offset, half, arriving=True).wait_recv()

    def run(chip, rows, count):
        piece = xbuf[pl.ds(chip * 2, 2), rows].reshape(2 * count, width)
        gated = dot32(piece, gate[0])
        upward = dot32(piece, up[0])
        hidden = (jax.nn.silu(gated) * upward).astype(jnp.bfloat16)
        for begin in range(0, width, 512):
            cols = slice(begin, begin + 512)
            term = dot32(hidden, down[0, :, cols]).astype(jnp.bfloat16)
            pbuf[pl.ds(chip * 2, 2), rows, cols] = term.reshape(2, count, 512)

    def experts(first, count):
        def step(number, carry):
            run(ex.chip(first - 2 * first * number), pl.ds(0, 2 * part), 2 * part)
            return carry

        lax.fori_loop(0, count, step, 0)

    def experts_halves(first):
        def step(number, carry):
            chip = ex.chip(first - 2 * first * number)
            run(chip, pl.ds(pl.multiple_of(number * part, part), part), part)
            return carry

        lax.fori_loop(0, 2, step, 0)

    for way in range(2):
        ag_copy(way, way, 0).start()
        ag_copy(way, 1 - way, 0).start()
    for half in range(2):
        share_copy(0, half).start()
    for load in weight_loads(gate_hbm, up_hbm, down_hbm, gate, up, down, w_sem):
        load.wait()
    feed(0)
    experts(0, 1)
    ex.give(0)
    for distance in (1, 2):
        came(0, 0, distance)
        came(1, 1, distance)
        came(0, 1, distance)
        came(1, 0, distance)
        feed(-distance)
        feed(distance)
        experts(distance, 2)
        ex.give(-distance, distance)
    came(0, 0, 3)
    came(1, 1, 3)
    feed_half(-3, 0)
    feed_half(3, 1)
    experts_halves(-3)
    ex.pair_copy(-3, 0).start()
    ex.pair_copy(3, 1).start()
    came(0, 1, 3)
    came(1, 0, 3)
    ex.pair_copy(3, 1).wait_recv()
    ex.send(0, 1, 3)
    ex.pair_copy(-3, 0).wait_recv()
    ex.send(1, 0, 3)
    feed_half(3, 0)
    feed_half(-3, 1)
    experts_halves(3)
    ex.pair_copy(3, 0).start()
    ex.pair_copy(-3, 1).start()
    came(0, 0, 4)
    came(1, 1, 4)
    feed(4)
    experts(4, 1)
    ex.give(4)
    ex.take(4)
    ex.send(0, 0, 4)
    ex.send(1, 1, 4)
    ex.pair_copy(3, 0).wait_recv()
    ex.pair_copy(-3, 1).wait_recv()
    ex.take(2, -2, 1, -1, 0)
    for distance in (3, 2, 1):
        if distance < 3:
            ex.send(0, 1, distance)
            ex.send(1, 0, distance)
        ex.send(0, 0, distance)
        ex.send(1, 1, distance)
    widen = unpacking(part, capacity)
    for half in range(2):
        summed = ex.last(half).astype(jnp.bfloat16)
        spread = dot32(widen, summed).astype(jnp.bfloat16)
        returned[half * 8 : half * 8 + 8] = spread.reshape(8, SLAB, width)
    for delta in range(1, 16):
        slab_copy(returned, back, delta, back_send, back_recv).start()
    back[sp] = returned[sp]
    tokens = mixed.shape[0]
    row = lax.broadcasted_iota(jnp.int32, (tokens, tokens), 0)
    same = row == lax.broadcasted_iota(jnp.int32, (tokens, tokens), 1)
    picks = [jnp.transpose(c.astype(jnp.float32)).astype(jnp.bfloat16) for c in chosen]
    factors = [
        jnp.sum(jnp.where(same, weights_ref[r : r + 1, :], 0.0), axis=1, keepdims=True)
        for r in range(2)
    ]
    for delta in range(1, 16):
        slab_copy(returned, back, delta, back_send, back_recv, arriving=True).wait_recv()
    rows = back[...].reshape(16 * SLAB, width)
    added = factors[0] * dot32(picks[0], rows) + factors[1] * dot32(picks[1], rows)
    out_ref[...] = (mixed[...] + added).astype(jnp.bfloat16)
    for delta in range(1, 16):
        slab_copy(slabs, landing, delta, go_send, go_recv).wait_send()
        slab_copy(returned, back, delta, back_send, back_recv).wait_send()
    px.finish()
    ex.finish()
    for way in range(2):
        for half in range(2):
            for distance in range(4 if half == way else 3):
                ag_copy(way, half, distance).wait_send()
    for offset in range(-3, 5):
        for half in range(2):
            share_copy(offset, half).wait_send()


def weight_loads(gate_hbm, up_hbm, down_hbm, gate, up, down, w_sem):
    pairs = ((gate_hbm, gate), (up_hbm, up), (down_hbm, down))
    return [pltpu.make_async_copy(a, b, w_sem.at[i]) for i, (a, b) in enumerate(pairs)]


ATTENTION_INPUTS, ATTENTION_SCRATCH = 10, 18


def whole_kernel(*refs):
    inputs, (out_ref, heads), scratch = refs[:19], refs[19:21], refs[21:]
    own, rest = scratch[:ATTENTION_SCRATCH], scratch[ATTENTION_SCRATCH:]
    for load in weight_loads(*inputs[16:19], *rest[10:14]):
        load.start()
    finish = attention_part(*inputs[:ATTENTION_INPUTS], heads, *own)
    experts_part(heads, *inputs[ATTENTION_INPUTS:], out_ref, *rest)
    finish()


def per_device(
    resid,
    query_a,
    key_a,
    value_a,
    query_b,
    key_b,
    value_b,
    mix_a,
    mix_b,
    head_gain_a,
    head_gain_b,
    proj_a,
    proj_b,
    norm_gain,
    route_ids,
    route_weights,
    expert_gate,
    expert_up,
    expert_down,
):
    tokens, width = resid.shape
    rows = query_a.shape[0]
    half = rows // 2
    count = 3 * route_ids.shape[1] * tokens // 2
    vmem = pl.BlockSpec(memory_space=pltpu.VMEM)
    smem = pl.BlockSpec(memory_space=pltpu.SMEM)
    anywhere = pl.BlockSpec(memory_space=pl.ANY)
    attention_scratch = [
        pltpu.VMEM((16, 2, half, 384), jnp.bfloat16),
        pltpu.VMEM((4, 128, half), jnp.bfloat16),
        pltpu.VMEM((4, 64, half), jnp.bfloat16),
        pltpu.VMEM((2, half, 64), jnp.bfloat16),
        *[pltpu.VMEM((rows, half), jnp.float32)] * 4,
        *[pltpu.VMEM((rows, half), jnp.bfloat16)] * 4,
        pltpu.VMEM((4, 128, half), jnp.float32),
        pltpu.VMEM((4, 64, half), jnp.float32),
        pltpu.VMEM((8, 1, half), jnp.float32),
        pltpu.VMEM((8, 8, half), jnp.float32),
        pltpu.SemaphoreType.DMA((40,)),
        pltpu.SemaphoreType.DMA((40,)),
    ]
    experts_scratch = [
        pltpu.VMEM((tokens, width), jnp.float32),
        *[pltpu.VMEM((16, SLAB, width), jnp.bfloat16)] * 4,
        *[pltpu.SemaphoreType.DMA((16,))] * 4,
        pltpu.VMEM((16, count, width), jnp.bfloat16),
        pltpu.VMEM(expert_gate.shape, expert_gate.dtype),
        pltpu.VMEM(expert_up.shape, expert_up.dtype),
        pltpu.VMEM(expert_down.shape, expert_down.dtype),
        pltpu.SemaphoreType.DMA((3,)),
        *[pltpu.SemaphoreType.DMA((16,))] * 4,
        *exchange_scratch(tokens, width),
        *exchange_scratch(count, width),
    ]
    return pl.pallas_call(
        whole_kernel,
        out_shape=jax.ShapeDtypeStruct((tokens, width), jnp.bfloat16),
        in_specs=[vmem] * 6 + [smem] * 2 + [vmem] * 8 + [anywhere] * 3,
        out_specs=vmem,
        scratch_shapes=[pltpu.VMEM((rows, 192), jnp.bfloat16), *attention_scratch, *experts_scratch],
        compiler_params=pltpu.CompilerParams(
            collective_id=0, has_side_effects=True, vmem_limit_bytes=60 * 1024 * 1024
        ),
    )(
        query_a[:, 0, :], query_b[:, 0, :].T, key_a[:, 0, :], value_a[:, 0, :],
        key_b[:, 0, :].T, value_b[:, 0, :].T,
        mix_a, mix_b, head_gain_a[None, :], head_gain_b[None, :],
        proj_a, proj_b, resid, norm_gain[None, :], route_ids.T, route_weights.T,
        expert_gate, expert_up, expert_down,
    )


def solution(mesh):
    placed = (
        P(("sp", "tp"), None),
        P("sp", "tp", None),
        P("sp", "tp", None),
        P("sp", "tp", None),
        P("sp", "tp", None),
        P("sp", "tp", None),
        P("sp", "tp", None),
        P("tp"),
        P("tp"),
        P(),
        P(),
        P("tp", None),
        P("tp", None),
        P(),
        P(("sp", "tp"), None),
        P(("sp", "tp"), None),
        P("sp", None, "tp"),
        P("sp", None, "tp"),
        P("sp", "tp", None),
    )
    return jax.shard_map(
        per_device, mesh=mesh, in_specs=placed, out_specs=P(("sp", "tp"), None), check_vma=False
    )
```

```python
import math

import jax
import jax.numpy as jnp
from jax import lax
from jax.experimental import pallas as pl
from jax.experimental.pallas import tpu as pltpu
from jax.sharding import PartitionSpec as P

EPS = 1e-06
NEG = -1e30
HEAD_SCALE = 1.0 - (0.8 - 0.6 * math.exp(-0.3))


def rms_scaled(values, gain):
    return values * lax.rsqrt(jnp.mean(values * values, axis=-1, keepdims=True) + EPS) * gain


MESH = pl.DeviceIdType.MESH
LOG2E = 1.4426950408889634
PART = 128
CHUNK = 32
PIECES = 4


def dot32(a, b):
    return jnp.dot(a, b, preferred_element_type=jnp.float32)


def attention_part(
    qa_ref, qb_ref, ka_ref, va_ref, kb_ref, vb_ref, mix_a_ref, mix_b_ref, gain_a_ref, gain_b_ref,
    out_ref,
    buf, qta, qtb, k_b, s_0, s_1, s_2, s_3, p_0, p_1, p_2, p_3, acc_a, acc_b, m_ref, l_ref,
    send_sem, recv_sem,
):
    s_refs, p_refs = (s_0, s_1, s_2, s_3), (p_0, p_1, p_2, p_3)
    place = lax.axis_index("sp")
    tp = lax.axis_index("tp")
    y, x = place // 4, place % 4
    half = buf.shape[2]

    def at(ox, oy):
        return ((y + oy + 4) % 4) * 4 + (x + ox + 4) % 4

    def spot(h, df, dg):
        return at(df, dg) if h == 0 else at(dg, df)

    peers = greet()

    va_t = jnp.transpose(va_ref[...])
    for h in range(2):
        cols = slice(h * half, (h + 1) * half)
        buf[place, h, :, 0:128] = ka_ref[cols, :]
        buf[place, h, 0:128, 128:384] = va_t[:, cols]
        buf[place, h, 128:192, 128:384] = kb_ref[:, cols]
        buf[place, h, 192:256, 128:384] = vb_ref[:, cols]

    pl.semaphore_wait(pltpu.get_barrier_semaphore(), peers)

    def region(h, df, dg, part):
        ref = buf.at[spot(h, df, dg), h]
        return ref if part is None else ref.at[pl.ds(part * PART, PART)]

    def copy(h, number, df, dg, part, to_f, to_g):
        ref = region(h, df, dg, part)
        return pltpu.make_async_remote_copy(
            src_ref=ref,
            dst_ref=ref,
            send_sem=send_sem.at[h * 20 + number],
            recv_sem=recv_sem.at[h * 20 + number],
            device_id=(spot(h, to_f, to_g), tp),
            device_id_type=MESH,
        )

    moves = {
        0: (0, 0, None, 1, 0), 1: (0, 0, None, -1, 0),
        2: (0, 0, None, 0, 1), 3: (0, 0, None, 0, -1),
        4: (-1, 0, 0, 1, 0), 5: (1, 0, 1, -1, 0),
        6: (-1, 0, None, 0, 1), 7: (-1, 0, None, 0, -1),
        8: (1, 0, None, 0, 1), 9: (1, 0, None, 0, -1),
        10: (2, 0, None, 0, 1), 11: (2, 0, None, 0, -1),
        12: (0, -1, 0, 0, 1), 13: (0, 1, 1, 0, -1),
        14: (-1, -1, 0, 0, 1), 15: (-1, 1, 1, 0, -1),
        16: (1, -1, 0, 0, 1), 17: (1, 1, 1, 0, -1),
        18: (2, -1, 0, 0, 1), 19: (2, 1, 1, 0, -1),
    }

    def start(*numbers):
        for number in numbers:
            for h in range(2):
                copy(h, number, *moves[number]).start()

    def arrive(number, *then):
        df, dg, part, to_f, to_g = moves[number]
        for h in range(2):
            copy(h, number, df - to_f, dg - to_g, part, to_f, to_g).wait_recv()
            for follow in then:
                copy(h, follow, *moves[follow]).start()

    start(0, 1, 2, 3)

    qa_t = jnp.transpose(qa_ref[...])
    zero_a = jnp.zeros((64, half), jnp.bfloat16)
    zero_b = jnp.zeros((32, half), jnp.bfloat16)
    for h in range(2):
        cols = slice(h * half, (h + 1) * half)
        qta[h, 0:64, :] = qa_t[0:64, cols]
        qta[h, 64:128, :] = zero_a
        qta[2 + h, 0:64, :] = zero_a
        qta[2 + h, 64:128, :] = qa_t[64:128, cols]
        qtb[h, 0:32, :] = qb_ref[0:32, cols]
        qtb[h, 32:64, :] = zero_b
        qtb[2 + h, 0:32, :] = zero_b
        qtb[2 + h, 32:64, :] = qb_ref[32:64, cols]
    acc_a[...] = jnp.zeros_like(acc_a)
    acc_b[...] = jnp.zeros_like(acc_b)
    m_ref[...] = jnp.full_like(m_ref, NEG)
    l_ref[...] = jnp.zeros_like(l_ref)

    def score(number, source, offsets):
        index, group, place_in = number // 2, number % 2, number % 2
        top = None
        for h in range(2):
            keys = k_b[h] if group else buf[source, h, :, 0:128]
            found = dot32(keys, qtb[index] if group else qta[index])
            if offsets is not None:
                query_pos = (index % 2) * half + lax.broadcasted_iota(jnp.int32, (half, half), 1)
                key_pos = offsets[h] + lax.broadcasted_iota(jnp.int32, (half, half), 0)
                found = jnp.where(key_pos <= query_pos, found, NEG)
            s_refs[number % 4][h * half : (h + 1) * half, :] = found
            most = jnp.max(found.reshape(half // 8, 8, half), axis=0)
            top = most if top is None else jnp.maximum(top, most)
        return jnp.max(top, axis=0, keepdims=True)

    def soften(number, top):
        index, group = number // 2, number % 2
        slot, factor = index + 4 * group, (LOG2E / math.sqrt(32.0) if group else LOG2E / 8.0)
        old = m_ref[slot]
        fresh = jnp.maximum(old, top)
        scale = jnp.exp2((old - fresh) * factor)
        m_ref[slot] = fresh
        sums = l_ref[slot] * scale
        for first in range(0, 2 * half, CHUNK):
            rows = slice(first, first + CHUNK)
            weights = jnp.exp2((s_refs[number % 4][rows, :] - fresh) * factor)
            sums = sums + jnp.sum(weights.reshape(CHUNK // 8, 8, half), axis=0)
            p_refs[number % 4][rows, :] = weights.astype(jnp.bfloat16)
        l_ref[slot] = sums
        return scale

    def gather(number, source, scale):
        index, group = number // 2, number % 2
        acc, rows = (acc_b, slice(192, 256)) if group else (acc_a, slice(0, 128))
        added = dot32(buf[source, 0, rows, 128:384], p_refs[number % 4][0:half, :])
        added = added + dot32(buf[source, 1, rows, 128:384], p_refs[number % 4][half : 2 * half, :])
        acc[index] = acc[index] * scale + added

    def block(source, offsets):
        for h in range(2):
            k_b[h] = jnp.transpose(buf[source, h, 128:192, 128:384])
        tops = [score(number, source, offsets) for number in range(2)]
        for number in range(8):
            if number + 2 < 8:
                tops.append(score(number + 2, source, offsets))
            gather(number, source, soften(number, tops[number]))

    plan = (
        ((-1, 0), ()), ((0, -1), (4, 5)), ((1, 0), ()), ((0, 1), (6, 7)), ((-1, -1), ()),
        ((2, 0), (12, 13)), ((0, 2), (8, 9)), ((1, -1), ()), ((-1, 1), ()), ((1, 1), ()),
        ((2, -1), (10, 11, 14, 15)), ((-1, 2), (16, 17)), ((2, 1), ()), ((1, 2), (18, 19)),
        ((2, 2), ()),
    )
    follow = {5: (10, 11), 6: (14,), 7: (15,), 8: (16,), 9: (17,), 10: (18,), 11: (19,)}

    def step(number, carry):
        ox, oy = jnp.int32(0), jnp.int32(0)
        for which, ((dx, dy), events) in enumerate(plan):
            ox = jnp.where(number == which, dx, ox)
            oy = jnp.where(number == which, dy, oy)
            if events:

                @pl.when(number == which)
                def _(events=events):
                    for event in events:
                        arrive(event, *follow.get(event, ()))

        source = at(ox, oy)

        @pl.when(source < place)
        def _():
            block(source, None)

        return carry

    block(place, (0, half))
    arrive(0, 4, 6, 7)
    arrive(1, 5)
    arrive(2, 12)
    arrive(3, 13, 8, 9)
    lax.fori_loop(0, len(plan), step, 0)

    for h in range(2):
        for acc, base, mix, gain, first in (
            (acc_a, 0, mix_a_ref, gain_a_ref, 0), (acc_b, 4, mix_b_ref, gain_b_ref, 128),
        ):
            one = acc[h] / jnp.sum(l_ref[base + h], axis=0, keepdims=True)
            two = acc[2 + h] / jnp.sum(l_ref[base + 2 + h], axis=0, keepdims=True)
            mixed = one - mix[0] * two
            mixed = mixed * lax.rsqrt(jnp.mean(mixed * mixed, axis=0, keepdims=True) + EPS)
            rows = jnp.transpose(mixed) * gain[...] * HEAD_SCALE
            out_ref[h * half : (h + 1) * half, first : first + rows.shape[1]] = rows.astype(
                jnp.bfloat16
            )

    def finish():
        for number in range(20):
            for h in range(2):
                copy(h, number, *moves[number]).wait_send()

    return finish


def tp_place():
    tp = lax.axis_index("tp")
    return lax.axis_index("sp"), tp // 2, tp % 2


def greet():
    sp, z, core = tp_place()
    tp = z * 2 + core
    barrier = pltpu.get_barrier_semaphore()
    peers = [(sp, ((z + 1) % 8) * 2 + core), (sp, ((z + 7) % 8) * 2 + core), (sp, tp + 1 - 2 * core)]
    peers += [((sp + delta) % 16, tp) for delta in range(1, 16)]
    for peer in peers:
        pl.semaphore_signal(barrier, inc=1, device_id=peer, device_id_type=MESH)
    return len(peers)


class Exchange:
    def __init__(self, pbuf, other, stage, landed, pair_send, pair_recv, ring_send, ring_recv):
        self.sp, self.z, self.core = tp_place()
        self.pbuf, self.other, self.stage, self.landed = pbuf, other, stage, landed
        self.pair_sems, self.ring_sems = (pair_send, pair_recv), (ring_send, ring_recv)
        self.rows, self.wide = pbuf.shape[1] // 2, pbuf.shape[2] // PIECES

    def chip(self, offset):
        return (self.z + offset + 8) % 8

    def pair_copy(self, offset, half):
        chip = self.chip(offset)
        rows = pl.ds(half * self.rows, self.rows)
        number = (offset + 3) * 2 + half
        return pltpu.make_async_remote_copy(
            src_ref=self.pbuf.at[chip * 2 + 1 - self.core, rows],
            dst_ref=self.other.at[chip, rows],
            send_sem=self.pair_sems[0].at[number],
            recv_sem=self.pair_sems[1].at[number],
            device_id=(self.sp, self.z * 2 + 1 - self.core),
            device_id_type=MESH,
        )

    def give(self, *offsets):
        for offset in offsets:
            for half in range(2):
                self.pair_copy(offset, half).start()

    def take(self, *offsets):
        for offset in offsets:
            for half in range(2):
                self.pair_copy(offset, half).wait_recv()

    def ring_copy(self, way, half, distance, piece):
        number = ((way * 2 + half) * 4 + distance - 1) * PIECES + piece
        columns = pl.ds(piece * self.wide, self.wide)
        return pltpu.make_async_remote_copy(
            src_ref=self.stage.at[way, half, distance - 1, :, columns],
            dst_ref=self.landed.at[way, half, distance - 1, :, columns],
            send_sem=self.ring_sems[0].at[number],
            recv_sem=self.ring_sems[1].at[number],
            device_id=(self.sp, self.chip(1 - 2 * way) * 2 + self.core),
            device_id_type=MESH,
        )

    def mine(self, offset, half, columns=slice(None)):
        chip = self.chip(offset)
        rows = slice(half * self.rows, (half + 1) * self.rows)
        own = self.pbuf[chip * 2 + self.core, rows, columns].astype(jnp.float32)
        return own + self.other[chip, rows, columns].astype(jnp.float32)

    def send(self, way, half, distance):
        offset = distance * (1 - 2 * way)
        for piece in range(PIECES):
            columns = slice(piece * self.wide, (piece + 1) * self.wide)
            total = self.mine(4 if distance == 4 else offset, half, columns)
            if distance < (4 if half == way else 3):
                self.ring_copy(way, half, distance + 1, piece).wait_recv()
                total = total + self.landed[way, half, distance, :, columns].astype(jnp.float32)
            self.stage[way, half, distance - 1, :, columns] = total.astype(jnp.bfloat16)
            self.ring_copy(way, half, distance, piece).start()

    def last(self, half):
        total = self.mine(0, half)
        for way in range(2):
            for piece in range(PIECES):
                self.ring_copy(way, half, 1, piece).wait_recv()
            total = total + self.landed[way, half, 0].astype(jnp.float32)
        return total

    def finish(self):
        for offset in range(-3, 5):
            for half in range(2):
                self.pair_copy(offset, half).wait_send()
        for way in range(2):
            for half in range(2):
                for distance in range(1, 5 if half == way else 4):
                    for piece in range(PIECES):
                        self.ring_copy(way, half, distance, piece).wait_send()


def exchange_scratch(rows, width):
    return [
        pltpu.VMEM((16, rows, width), jnp.bfloat16),
        pltpu.VMEM((8, rows, width), jnp.bfloat16),
        pltpu.VMEM((2, 2, 4, rows // 2, width), jnp.bfloat16),
        pltpu.VMEM((2, 2, 4, rows // 2, width), jnp.bfloat16),
        pltpu.SemaphoreType.DMA((16,)),
        pltpu.SemaphoreType.DMA((16,)),
        pltpu.SemaphoreType.DMA((16 * PIECES,)),
        pltpu.SemaphoreType.DMA((16 * PIECES,)),
    ]


SLAB = 8


def slab_copy(slabs, landing, delta, send_sem, recv_sem, arriving=False):
    sp, tp = lax.axis_index("sp"), lax.axis_index("tp")
    there = (sp + delta) % 16
    return pltpu.make_async_remote_copy(
        src_ref=slabs.at[there],
        dst_ref=landing.at[(sp + 16 - delta) % 16 if arriving else sp],
        send_sem=send_sem.at[delta],
        recv_sem=recv_sem.at[delta],
        device_id=(there, tp),
        device_id_type=MESH,
    )


def chosen_slots(ids_ref):
    tokens = ids_ref.shape[1]
    expert = lax.broadcasted_iota(jnp.int32, (16, tokens), 0)
    named = [(expert == ids_ref[r : r + 1, :]).astype(jnp.float32) for r in range(2)]
    earlier = lax.broadcasted_iota(jnp.int32, (tokens, tokens), 0)
    earlier = (earlier < lax.broadcasted_iota(jnp.int32, (tokens, tokens), 1)).astype(jnp.bfloat16)
    before = dot32((named[0] + named[1]).astype(jnp.bfloat16), earlier)
    slots = lax.broadcasted_iota(jnp.int32, (16 * SLAB, tokens), 0)
    result = []
    for r in range(2):
        rank = jnp.sum(named[r] * before, axis=0, keepdims=True).astype(jnp.int32)
        result.append((slots == ids_ref[r : r + 1, :] * SLAB + rank).astype(jnp.bfloat16))
    return result


def packing(rows, capacity):
    shape = (rows, rows // capacity * SLAB)
    row = lax.broadcasted_iota(jnp.int32, shape, 0)
    column = lax.broadcasted_iota(jnp.int32, shape, 1)
    used = column % SLAB < capacity
    return (used & (row == column // SLAB * capacity + column % SLAB)).astype(jnp.bfloat16)


def unpacking(rows, capacity):
    shape = (rows // capacity * SLAB, rows)
    row = lax.broadcasted_iota(jnp.int32, shape, 0)
    column = lax.broadcasted_iota(jnp.int32, shape, 1)
    used = row % SLAB < capacity
    return (used & (column == row // SLAB * capacity + row % SLAB)).astype(jnp.bfloat16)


def experts_part(
    heads_ref, proj_a_ref, proj_b_ref, resid_ref, gain_ref, ids_ref, weights_ref,
    gate_hbm, up_hbm, down_hbm, out_ref,
    mixed, slabs, landing, returned, back, go_send, go_recv, back_send, back_recv,
    xbuf, gate, up, down, w_sem, ag_send, ag_recv, share_send, share_recv, *exchange,
):
    sp, z, core = tp_place()
    px = Exchange(*exchange[:8])
    ex = Exchange(*exchange[8:])
    width = mixed.shape[1]
    pbuf = ex.pbuf
    for first in range(0, width, 512):
        cols = slice(first, first + 512)
        term = dot32(heads_ref[:, 0:128], proj_a_ref[:, cols])
        term = term + dot32(heads_ref[:, 128:192], proj_b_ref[:, cols])
        px.pbuf[:, :, cols] = term.astype(jnp.bfloat16).reshape(16, 32, 512)
    px.give(4, 3, -3, 2, -2, 1, -1, 0)
    chosen = chosen_slots(ids_ref)
    px.take(4)
    px.send(0, 0, 4)
    px.send(1, 1, 4)
    for distance in (3, 2, 1):
        px.take(distance, -distance)
        if distance == 3:
            px.send(0, 1, 3)
            px.send(1, 0, 3)
        px.send(0, 0, distance)
        px.send(1, 1, distance)
        if distance < 3:
            px.send(0, 1, distance)
            px.send(1, 0, distance)
    px.take(0)
    for half in range(2):
        rows = slice(half * 16, half * 16 + 16)
        mixed[rows, :] = resid_ref[rows, :].astype(jnp.float32) + px.last(half)
    normed = rms_scaled(mixed[...], gain_ref[...]).astype(jnp.bfloat16)
    outgoing = dot32(chosen[0] + chosen[1], normed).astype(jnp.bfloat16)
    slabs[...] = outgoing.reshape(16, SLAB, width)
    for delta in range(1, 16):
        slab_copy(slabs, landing, delta, go_send, go_recv).start()
    landing[sp] = slabs[sp]
    for delta in range(1, 16):
        slab_copy(slabs, landing, delta, go_send, go_recv, arriving=True).wait_recv()
    count = xbuf.shape[1]
    capacity = count // 16
    arrived = landing[...].reshape(16 * SLAB, width)
    xbuf[z * 2 + core] = dot32(packing(count, capacity), arrived).astype(jnp.bfloat16)
    part = count // 2

    def shard(offset, half):
        chip = ex.chip(offset)
        return xbuf.at[chip * 2 + core, pl.ds(half * part, part)]

    def ag_copy(way, half, distance, arriving=False):
        sign = 1 - 2 * way
        away = distance + 1 if arriving else distance
        offset = 4 if away == 4 else -sign * away
        number = way * 8 + half * 4 + distance
        return pltpu.make_async_remote_copy(
            src_ref=shard(offset, half),
            dst_ref=shard(offset, half),
            send_sem=ag_send.at[number],
            recv_sem=ag_recv.at[number],
            device_id=(sp, ex.chip(sign) * 2 + core),
            device_id_type=MESH,
        )

    def share_copy(offset, half, arriving=False):
        chip = ex.chip(offset)
        there = xbuf.at[chip * 2 + (1 - core if arriving else core), pl.ds(half * part, part)]
        number = (offset + 3) * 2 + half
        return pltpu.make_async_remote_copy(
            src_ref=there,
            dst_ref=there,
            send_sem=share_send.at[number],
            recv_sem=share_recv.at[number],
            device_id=(sp, z * 2 + 1 - core),
            device_id_type=MESH,
        )

    def came(way, half, distance):
        ag_copy(way, half, distance - 1, arriving=True).wait_recv()
        if distance < (4 if half == way else 3):
            ag_copy(way, half, distance).start()
        offset = 4 if distance == 4 else -distance * (1 - 2 * way)
        share_copy(offset, half).start()

    def feed(offset):
        for half in range(2):
            share_copy(offset, half, arriving=True).wait_recv()

    def feed_half(offset, half):
        share_copy(offset, half, arriving=True).wait_recv()

    def run(chip, rows, count):
        piece = xbuf[pl.ds(chip * 2, 2), rows].reshape(2 * count, width)
        gated = dot32(piece, gate[0])
        upward = dot32(piece, up[0])
        hidden = (jax.nn.silu(gated) * upward).astype(jnp.bfloat16)
        for begin in range(0, width, 512):
            cols = slice(begin, begin + 512)
            term = dot32(hidden, down[0, :, cols]).astype(jnp.bfloat16)
            pbuf[pl.ds(chip * 2, 2), rows, cols] = term.reshape(2, count, 512)

    def experts(first, count):
        def step(number, carry):
            run(ex.chip(first - 2 * first * number), pl.ds(0, 2 * part), 2 * part)
            return carry

        lax.fori_loop(0, count, step, 0)

    def experts_halves(first):
        def step(number, carry):
            chip = ex.chip(first - 2 * first * number)
            run(chip, pl.ds(pl.multiple_of(number * part, part), part), part)
            return carry

        lax.fori_loop(0, 2, step, 0)

    for way in range(2):
        ag_copy(way, way, 0).start()
        ag_copy(way, 1 - way, 0).start()
    for half in range(2):
        share_copy(0, half).start()
    for load in weight_loads(gate_hbm, up_hbm, down_hbm, gate, up, down, w_sem):
        load.wait()
    feed(0)
    experts(0, 1)
    ex.give(0)
    for distance in (1, 2):
        came(0, 0, distance)
        came(1, 1, distance)
        came(0, 1, distance)
        came(1, 0, distance)
        feed(-distance)
        feed(distance)
        experts(distance, 2)
        ex.give(-distance, distance)
    came(0, 0, 3)
    came(1, 1, 3)
    feed_half(-3, 0)
    feed_half(3, 1)
    experts_halves(-3)
    ex.pair_copy(-3, 0).start()
    ex.pair_copy(3, 1).start()
    came(0, 1, 3)
    came(1, 0, 3)
    ex.pair_copy(3, 1).wait_recv()
    ex.send(0, 1, 3)
    ex.pair_copy(-3, 0).wait_recv()
    ex.send(1, 0, 3)
    feed_half(3, 0)
    feed_half(-3, 1)
    experts_halves(3)
    ex.pair_copy(3, 0).start()
    ex.pair_copy(-3, 1).start()
    came(0, 0, 4)
    came(1, 1, 4)
    feed(4)
    experts(4, 1)
    ex.give(4)
    ex.take(4)
    ex.send(0, 0, 4)
    ex.send(1, 1, 4)
    ex.pair_copy(3, 0).wait_recv()
    ex.pair_copy(-3, 1).wait_recv()
    ex.take(2, -2, 1, -1, 0)
    for distance in (3, 2, 1):
        if distance < 3:
            ex.send(0, 1, distance)
            ex.send(1, 0, distance)
        ex.send(0, 0, distance)
        ex.send(1, 1, distance)
    widen = unpacking(part, capacity)
    for half in range(2):
        summed = ex.last(half).astype(jnp.bfloat16)
        spread = dot32(widen, summed).astype(jnp.bfloat16)
        returned[half * 8 : half * 8 + 8] = spread.reshape(8, SLAB, width)
    for delta in range(1, 16):
        slab_copy(returned, back, delta, back_send, back_recv).start()
    back[sp] = returned[sp]
    tokens = mixed.shape[0]
    row = lax.broadcasted_iota(jnp.int32, (tokens, tokens), 0)
    same = row == lax.broadcasted_iota(jnp.int32, (tokens, tokens), 1)
    picks = [jnp.transpose(c.astype(jnp.float32)).astype(jnp.bfloat16) for c in chosen]
    factors = [
        jnp.sum(jnp.where(same, weights_ref[r : r + 1, :], 0.0), axis=1, keepdims=True)
        for r in range(2)
    ]
    for delta in range(1, 16):
        slab_copy(returned, back, delta, back_send, back_recv, arriving=True).wait_recv()
    rows = back[...].reshape(16 * SLAB, width)
    added = factors[0] * dot32(picks[0], rows) + factors[1] * dot32(picks[1], rows)
    out_ref[...] = mixed[...] + added
    for delta in range(1, 16):
        slab_copy(slabs, landing, delta, go_send, go_recv).wait_send()
        slab_copy(returned, back, delta, back_send, back_recv).wait_send()
    px.finish()
    ex.finish()
    for way in range(2):
        for half in range(2):
            for distance in range(4 if half == way else 3):
                ag_copy(way, half, distance).wait_send()
    for offset in range(-3, 5):
        for half in range(2):
            share_copy(offset, half).wait_send()


def weight_loads(gate_hbm, up_hbm, down_hbm, gate, up, down, w_sem):
    pairs = ((gate_hbm, gate), (up_hbm, up), (down_hbm, down))
    return [pltpu.make_async_copy(a, b, w_sem.at[i]) for i, (a, b) in enumerate(pairs)]


ATTENTION_INPUTS, ATTENTION_SCRATCH = 10, 18


def whole_kernel(*refs):
    inputs, (out_ref, heads), scratch = refs[:19], refs[19:21], refs[21:]
    own, rest = scratch[:ATTENTION_SCRATCH], scratch[ATTENTION_SCRATCH:]
    for load in weight_loads(*inputs[16:19], *rest[10:14]):
        load.start()
    finish = attention_part(*inputs[:ATTENTION_INPUTS], heads, *own)
    experts_part(heads, *inputs[ATTENTION_INPUTS:], out_ref, *rest)
    finish()


def per_device(
    resid,
    query_a,
    key_a,
    value_a,
    query_b,
    key_b,
    value_b,
    mix_a,
    mix_b,
    head_gain_a,
    head_gain_b,
    proj_a,
    proj_b,
    norm_gain,
    route_ids,
    route_weights,
    expert_gate,
    expert_up,
    expert_down,
):
    tokens, width = resid.shape
    rows = query_a.shape[0]
    half = rows // 2
    count = 3 * route_ids.shape[1] * tokens // 2
    vmem = pl.BlockSpec(memory_space=pltpu.VMEM)
    smem = pl.BlockSpec(memory_space=pltpu.SMEM)
    anywhere = pl.BlockSpec(memory_space=pl.ANY)
    attention_scratch = [
        pltpu.VMEM((16, 2, half, 384), jnp.bfloat16),
        pltpu.VMEM((4, 128, half), jnp.bfloat16),
        pltpu.VMEM((4, 64, half), jnp.bfloat16),
        pltpu.VMEM((2, half, 64), jnp.bfloat16),
        *[pltpu.VMEM((rows, half), jnp.float32)] * 4,
        *[pltpu.VMEM((rows, half), jnp.bfloat16)] * 4,
        pltpu.VMEM((4, 128, half), jnp.float32),
        pltpu.VMEM((4, 64, half), jnp.float32),
        pltpu.VMEM((8, 1, half), jnp.float32),
        pltpu.VMEM((8, 8, half), jnp.float32),
        pltpu.SemaphoreType.DMA((40,)),
        pltpu.SemaphoreType.DMA((40,)),
    ]
    experts_scratch = [
        pltpu.VMEM((tokens, width), jnp.float32),
        *[pltpu.VMEM((16, SLAB, width), jnp.bfloat16)] * 4,
        *[pltpu.SemaphoreType.DMA((16,))] * 4,
        pltpu.VMEM((16, count, width), jnp.bfloat16),
        pltpu.VMEM(expert_gate.shape, expert_gate.dtype),
        pltpu.VMEM(expert_up.shape, expert_up.dtype),
        pltpu.VMEM(expert_down.shape, expert_down.dtype),
        pltpu.SemaphoreType.DMA((3,)),
        *[pltpu.SemaphoreType.DMA((16,))] * 4,
        *exchange_scratch(tokens, width),
        *exchange_scratch(count, width),
    ]
    output = pl.pallas_call(
        whole_kernel,
        out_shape=jax.ShapeDtypeStruct((tokens, width), jnp.float32),
        in_specs=[vmem] * 6 + [smem] * 2 + [vmem] * 8 + [anywhere] * 3,
        out_specs=vmem,
        scratch_shapes=[pltpu.VMEM((rows, 192), jnp.bfloat16), *attention_scratch, *experts_scratch],
        compiler_params=pltpu.CompilerParams(
            collective_id=0, has_side_effects=True, vmem_limit_bytes=60 * 1024 * 1024
        ),
    )(
        query_a[:, 0, :], query_b[:, 0, :].T, key_a[:, 0, :], value_a[:, 0, :],
        key_b[:, 0, :].T, value_b[:, 0, :].T,
        mix_a, mix_b, head_gain_a[None, :], head_gain_b[None, :],
        proj_a, proj_b, resid, norm_gain[None, :], route_ids.T, route_weights.T,
        expert_gate, expert_up, expert_down,
    )
    return output.astype(jnp.bfloat16)


def solution(mesh):
    placed = (
        P(("sp", "tp"), None),
        P("sp", "tp", None),
        P("sp", "tp", None),
        P("sp", "tp", None),
        P("sp", "tp", None),
        P("sp", "tp", None),
        P("sp", "tp", None),
        P("tp"),
        P("tp"),
        P(),
        P(),
        P("tp", None),
        P("tp", None),
        P(),
        P(("sp", "tp"), None),
        P(("sp", "tp"), None),
        P("sp", None, "tp"),
        P("sp", None, "tp"),
        P("sp", "tp", None),
    )
    return jax.shard_map(
        per_device, mesh=mesh, in_specs=placed, out_specs=P(("sp", "tp"), None), check_vma=False
    )
```
